1024 devices in a mesh: grp: 2 (over x), sp: 16 (over z), tp: 32 (over y, core).
Axes of the slice: x: 2, y: 16, z: 16, core: 2. Of those that a mesh axis runs over, the one named last changes fastest.
The devices are a block of a 4x16x16 slice.
Arguments:
- prompt_layer_input: bfloat16 [24, 2048, 2048], P('grp', 'sp'), parts along dimension 0, may hold values from -10 to 10
- next_token_input: bfloat16 [24, 2048], P('grp'), parts along dimension 0, may hold values from -6 to 6
- value_projection: bfloat16 [2048, 2048], P(None, 'tp'), may hold values from -0.125 to 0.125
- output_gate_matrix: bfloat16 [2048, 2048], P(None, 'tp'), may hold values from -0.125 to 0.125
- key_projection: bfloat16 [2048, 256], replicated, may hold values from -0.0390625 to 0.0390625
- query_projection: bfloat16 [2048, 256], replicated, may hold values from -0.125 to 0.125
- step_projection: bfloat16 [2048, 32], replicated, may hold values from -0.125 to 0.125
- value_filter_taps: bfloat16 [4, 2048], replicated, may hold values from -3 to 3
- key_filter_taps: bfloat16 [4, 256], replicated, may hold values from -3 to 3
- query_filter_taps: bfloat16 [4, 256], replicated, may hold values from -3 to 3
- step_size_bias: float32 [32], replicated, may hold values from -4.3 to -0.7
- head_decay_logarithm: float32 [32], replicated, may hold values from -8.5 to -0.5
- direct_path_weight: float32 [32], replicated, may hold values from 0.1 to 1.9
- gated_norm_gain: float32 [32, 64], replicated, may hold values from 0.1 to 1.9
- position_decay_offset: float32 [24, 2048, 32], P('grp', 'sp'), parts along dimension 0, may hold values from -2.1 to 0
Outputs:
- state_cache: bfloat16 [24, 32, 64, 128], P('grp', 'tp', 'sp'), parts along dimension 0
- first_read: bfloat16 [24, 32, 64], P('grp', 'tp', 'sp'), parts along dimension 0
The draws below stay inside these ranges and needn't reach their ends.
There are 2 independent parts, one for each index of `grp`. The reference program is written for one: setup_inputs(seed, part) draws one part's arguments, and reference() takes and returns one part's arrays. A program takes and returns all parts, laid end to end along the dimension named above; an argument that names none is the same for every part. Nothing has to cross between parts.
All inputs are finite; a program needn't handle non-finite values.
Results may differ from the reference program's by a relative error of at most 0.011.
Values may be sent and summed in bfloat16 or wider, within the bound.
No kernel may reach another device: no remote copies, remote signals or barrier semaphores. Data moves between devices by JAX's collectives and lax.ppermute only.
A program may use at most 32 MiB of HBM per device.

```python
import math
import jax
import jax.numpy as jnp
from jax import lax

D = 2048
HEADS = 32
P_SIZE = 64
GROUPS = 2
STATE = 128
CONV = 4
SPAN = 64
SEQS = 12
LEN = 2048


def head_speeds(key, fast_share):
    return jax.random.uniform(jax.random.fold_in(key, 11), (HEADS,), jnp.float32) < fast_share


def draw_step_size_bias(key, part):
    fast_share = 0.5
    fast_heads = head_speeds(key, fast_share)
    jitter = jax.random.uniform(jax.random.fold_in(key, 12), (HEADS,), jnp.float32, -0.3, 0.3)
    return (jnp.where(fast_heads, -1.0, -4.0) + jitter).astype(jnp.float32)


def draw_head_decay_logarithm(key, part):
    fast_share = 0.5
    fast_heads = head_speeds(key, fast_share)
    fraction = jax.random.uniform(jax.random.fold_in(key, 13), (HEADS,), jnp.float32)
    fast_rate = jnp.exp(math.log(0.01) + fraction * math.log(10.0 / 3.0)) / 0.4
    slow_rate = jnp.exp(math.log(0.1 / LEN) + fraction * math.log(6.0)) / 0.035
    return jnp.log(jnp.where(fast_heads, fast_rate, slow_rate)).astype(jnp.float32)


def draw_prompt_layer_input(key, part):
    block_count = LEN // SPAN
    drawn_draw = jnp.clip(jax.random.normal(jax.random.fold_in(key, 21), (SEQS, LEN, D), jnp.float32), -6.0, 6.0)
    spread = jnp.exp(jax.random.uniform(jax.random.fold_in(key, 22), (SEQS, block_count), jnp.float32, math.log(0.6), math.log(1.6)))
    shaped = drawn_draw.reshape(SEQS, block_count, SPAN, D) * spread[:, :, None, None]
    return shaped.reshape(SEQS, LEN, D).astype(jnp.bfloat16)


def draw_position_decay_offset(key, part):
    positions = jax.random.randint(jax.random.fold_in(key, 31), (SEQS, 3, HEADS), 0, LEN)
    strength = jax.random.uniform(jax.random.fold_in(key, 32), (SEQS, 3, HEADS), jnp.float32, math.log(0.5), math.log(0.8))
    places = jnp.arange(LEN, dtype=jnp.int32)
    matched = places[None, :, None, None] == positions[:, None, :, :]
    return jnp.sum(jnp.where(matched, strength[:, None], 0.0), axis=2).astype(jnp.float32)


def steps_of(own_key, dims, cuts, least, top_value):
    loudness = 1.0
    for axis_at, shards_of in cuts:
        heights = jax.random.uniform(jax.random.fold_in(jax.random.fold_in(own_key, 6), axis_at), (shards_of,), jnp.float32, least / len(cuts), top_value / len(cuts))
        loudness = loudness * jnp.repeat(jnp.exp(heights), dims[axis_at] // shards_of).reshape((-1,) + (1,) * (len(dims) - 1 - axis_at))
    return loudness


def gaussian(key, shape, scale, limit, cuts=(), kind=jnp.bfloat16):
    values = scale * jax.random.normal(key, shape, jnp.float32)
    if cuts:
        values = values * steps_of(key, shape, cuts, -0.22, 0.18)
    return jnp.clip(values, -limit, limit).astype(kind)


def setup_inputs(seed: int = 0, part: int = 0) -> dict:
    splits = jax.random.split(jax.random.key(seed), 16)
    part_keys = jax.random.split(jax.random.fold_in(splits[15], part), 16)
    return {
        "prompt_layer_input": draw_prompt_layer_input(jax.random.fold_in(jax.random.fold_in(splits[15], part), 71), part),
        "next_token_input": gaussian(part_keys[1], (SEQS, D), 1.0, 6.0),
        "value_projection": gaussian(splits[2], (D, HEADS * P_SIZE), D ** -0.5, 0.125, ((1, 32),)),
        "output_gate_matrix": gaussian(splits[3], (D, HEADS * P_SIZE), D ** -0.5, 0.125, ((1, 32),)),
        "key_projection": gaussian(splits[4], (D, GROUPS * STATE), (11 * D) ** -0.5, 0.0390625),
        "query_projection": gaussian(splits[5], (D, GROUPS * STATE), D ** -0.5, 0.125),
        "step_projection": gaussian(splits[6], (D, HEADS), D ** -0.5, 0.125),
        "value_filter_taps": gaussian(splits[7], (CONV, HEADS * P_SIZE), 0.5, 3.0),
        "key_filter_taps": gaussian(splits[8], (CONV, GROUPS * STATE), 0.5, 3.0),
        "query_filter_taps": gaussian(splits[9], (CONV, GROUPS * STATE), 0.5, 3.0),
        "step_size_bias": draw_step_size_bias(jax.random.fold_in(splits[15], 71), part),
        "head_decay_logarithm": draw_head_decay_logarithm(jax.random.fold_in(splits[15], 71), part),
        "direct_path_weight": jnp.clip(1.0 + 0.18 * jax.random.normal(splits[12], (HEADS,), jnp.float32), 0.1, 1.9),
        "gated_norm_gain": jnp.clip(1.0 + 0.18 * jax.random.normal(splits[13], (HEADS, P_SIZE), jnp.float32), 0.1, 1.9),
        "position_decay_offset": draw_position_decay_offset(jax.random.fold_in(jax.random.fold_in(splits[15], part), 71), part),
    }


epsilon = 1e-06

def reference(prompt_layer_input, next_token_input, value_projection, output_gate_matrix, key_projection, query_projection, step_projection, value_filter_taps, key_filter_taps, query_filter_taps, step_size_bias, head_decay_logarithm, direct_path_weight, gated_norm_gain, position_decay_offset):
    seq_count, length, width = prompt_layer_input.shape
    feature_cols = HEADS * P_SIZE
    map_cols = GROUPS * STATE
    weights_all = jnp.concatenate([value_projection, key_projection, query_projection], axis=1)
    kernel = jnp.concatenate([value_filter_taps, key_filter_taps, query_filter_taps], axis=1).astype(jnp.float32)
    token_rows = prompt_layer_input.reshape(seq_count * length, width)
    projected = jnp.dot(token_rows, weights_all, preferred_element_type=jnp.float32).astype(jnp.bfloat16)
    projected = projected.reshape(seq_count, length, feature_cols + 2 * map_cols)
    step_raw = jnp.dot(token_rows, step_projection, preferred_element_type=jnp.float32).astype(jnp.bfloat16)
    step_raw = step_raw.reshape(seq_count, length, HEADS)
    padded = jnp.concatenate([jnp.zeros((seq_count, CONV - 1, feature_cols + 2 * map_cols), jnp.bfloat16), projected], axis=1)
    total = padded[:, 0:length].astype(jnp.float32) * kernel[0]
    for tap in range(1, CONV):
        total = total + padded[:, tap:tap + length].astype(jnp.float32) * kernel[tap]
    mixed = jax.nn.silu(total).astype(jnp.bfloat16)
    head_decay_speed = jnp.exp(head_decay_logarithm)
    discrete_step = jax.nn.softplus(step_raw.astype(jnp.float32) + step_size_bias)
    logarithmic_decay = position_decay_offset - head_decay_speed * discrete_step
    head_input = mixed[:, :, :feature_cols].reshape(seq_count, length, HEADS, P_SIZE)
    in_map = mixed[:, :, feature_cols:feature_cols + map_cols].reshape(seq_count, length, GROUPS, STATE)
    block_count = length // SPAN

    def blocks(array):
        return jnp.moveaxis(array.reshape((seq_count, block_count, SPAN) + array.shape[2:]), 1, 0)

    def advance(carry, inputs):
        input_block, map_block, step_block, decay_block = inputs
        cumulative = jnp.cumsum(decay_block, axis=1)
        decay_weight = jnp.exp(cumulative[:, -1:] - cumulative) * step_block
        weighted = (input_block.astype(jnp.float32) * decay_weight[..., None]).astype(jnp.bfloat16)
        head_map = jnp.repeat(map_block, HEADS // GROUPS, axis=2)
        block_state = jnp.einsum('bshp,bshn->bhpn', weighted.astype(jnp.float32), head_map.astype(jnp.float32))
        return (jnp.exp(cumulative[:, -1])[:, :, None, None] * carry + block_state, None)
    final, unused = lax.scan(advance, jnp.zeros((seq_count, HEADS, P_SIZE, STATE), jnp.float32), (blocks(head_input), blocks(in_map), blocks(discrete_step), blocks(logarithmic_decay)))
    state_cache = final.astype(jnp.bfloat16)
    new_raw = jnp.dot(next_token_input, weights_all, preferred_element_type=jnp.float32).astype(jnp.bfloat16)
    new_step = jnp.dot(next_token_input, step_projection, preferred_element_type=jnp.float32).astype(jnp.bfloat16)
    new_gate = jnp.dot(next_token_input, output_gate_matrix, preferred_element_type=jnp.float32).astype(jnp.bfloat16)
    window = jnp.concatenate([projected[:, length - (CONV - 1):], new_raw[:, None]], axis=1)
    new_mixed = jax.nn.silu(lax.optimization_barrier(jnp.sum(window.astype(jnp.float32) * kernel[None], axis=1))).astype(jnp.bfloat16)
    new_input = new_mixed[:, :feature_cols].reshape(seq_count, HEADS, P_SIZE).astype(jnp.float32)
    new_in = jnp.repeat(new_mixed[:, feature_cols:feature_cols + map_cols].reshape(seq_count, GROUPS, STATE), HEADS // GROUPS, axis=1).astype(jnp.float32)
    new_out = jnp.repeat(new_mixed[:, feature_cols + map_cols:].reshape(seq_count, GROUPS, STATE), HEADS // GROUPS, axis=1).astype(jnp.float32)
    new_step_size = jax.nn.softplus(new_step.astype(jnp.float32) + step_size_bias)
    cache_values = lax.optimization_barrier(state_cache).astype(jnp.float32)
    new_state = jnp.exp(-head_decay_speed * new_step_size)[:, :, None, None] * cache_values + (new_step_size[:, :, None] * new_input)[..., None] * new_in[:, :, None, :]
    readout = lax.optimization_barrier(jnp.sum(new_state * new_out[:, :, None, :], axis=-1)) + direct_path_weight[None, :, None] * new_input
    gated = readout * jax.nn.silu(new_gate.astype(jnp.float32).reshape(seq_count, HEADS, P_SIZE))
    scale = lax.rsqrt(lax.optimization_barrier(jnp.mean(gated * gated, axis=(1, 2), keepdims=True)) + epsilon)
    first_read = (gated * scale * gated_norm_gain[None]).astype(jnp.bfloat16)
    return (state_cache, first_read)
```

```python
import jax
import jax.numpy as jnp
from jax import lax
from jax.experimental import pallas as pl
from jax.experimental.pallas import tpu as pltpu
from jax.sharding import Mesh
from jax.sharding import PartitionSpec as P

HEADS = 32
P_SIZE = 64
GROUPS = 2
STATE = 128
CONV = 4
LANES = 128
TP = ("tp_0", "tp_1")
EPSILON = 1e-06

F32 = jnp.float32
BF16 = jnp.bfloat16


def rounded(value):
    return value.astype(BF16).astype(F32)


def silu(value):
    return value / (1.0 + jnp.exp(-value))


def softplus(value):
    return jnp.maximum(value, 0.0) + jnp.log1p(jnp.exp(-jnp.abs(value)))


def dot(a, b, dims=((1,), (0,))):
    return lax.dot_general(a, b, (dims, ((), ())), preferred_element_type=F32)


def pieces(value):
    first = value.astype(BF16)
    rest = value - first.astype(F32)
    second = rest.astype(BF16)
    third = (rest - second.astype(F32)).astype(BF16)
    return first, second, third


def dot01(matrix, value):
    a, b, c = pieces(value)
    return dot(jnp.concatenate([matrix] * 3, axis=1), jnp.concatenate([a, b, c], axis=0))


def iota(shape, dim):
    return lax.broadcasted_iota(jnp.int32, shape, dim)


def own_half(row, head):
    return jnp.where(head % 2 == 0, row, pltpu.roll(row, 64, axis=1))


def pick(row, lane):
    return jnp.sum(jnp.where(iota(row.shape, 1) == lane, row, 0.0), axis=1, keepdims=True)


def pick_row(matrix, row):
    matrix = matrix.astype(F32)
    return jnp.sum(jnp.where(iota(matrix.shape, 0) == row, matrix, 0.0), axis=0, keepdims=True)


def local_body(
    x_hbm, value_ref, key_ref, step_ref, vt_ref, kt_ref, bias_ref, decay_ref, off_ref,
    state_ref, trail_ref, lead_ref, lead_weight_ref, logs_ref, taps_ref,
    x_ref, w_ref, trail_f32, sems, *, per,
):
    prompts, length, width = x_hbm.shape
    copies = []
    for i in range(prompts // per):
        part = pl.ds(i * per, per)
        copies.append(pltpu.make_async_copy(x_hbm.at[part], x_ref.at[part], sems.at[i]))
    for copy in copies:
        copy.start()
    head = lax.axis_index(TP)
    group = head // (HEADS // GROUPS)
    step_row = jnp.broadcast_to(pick_row(step_ref[...], head), (P_SIZE, width)).astype(BF16)
    w_ref[:, :LANES] = jnp.transpose(jnp.concatenate([value_ref[...], step_row], axis=0))
    trail_f32[...] = jnp.zeros_like(trail_f32)
    logs_ref[...] = jnp.zeros_like(logs_ref)
    at = pl.multiple_of(group * STATE, STATE)
    w_ref[:, LANES:] = key_ref[:, pl.ds(at, STATE)]
    pair = pl.multiple_of((head // 2) * LANES, LANES)
    value_taps = own_half(vt_ref[:, pl.ds(pair, LANES)].astype(F32), head)
    taps = jnp.concatenate([value_taps, kt_ref[:, pl.ds(at, STATE)].astype(F32)], axis=1)
    taps_ref[:CONV] = taps
    bias = pick(bias_ref[...], head)
    speed = jnp.exp(pick(decay_ref[...], head))
    later = (iota((length, length), 1) > iota((length, length), 0)).astype(BF16)
    position = iota((length, LANES), 0)
    for i in range(prompts // per):
        copies[i].wait()
        rows = x_ref[i * per : (i + 1) * per].reshape(per * length, width)
        raw_all = rounded(dot(rows, w_ref[...]))
        steps, logs, mixes = [], [], []
        for j in range(per):
            b = i * per + j
            raw = raw_all[j * length : (j + 1) * length]
            for k in range(CONV - 1):
                lead_ref[k, b : b + 1, :] = raw[k : k + 1]
                last = length - (CONV - 1) + k
                trail_f32[k, b : b + 1, :] = raw[last : last + 1]
            step = softplus(pltpu.roll(raw[:, :LANES], 64, axis=1) + bias)
            offset = jnp.broadcast_to(pick_row(off_ref[b], head), (length, length))
            log = jnp.transpose(offset) - speed * step
            total = raw * taps[CONV - 1 : CONV]
            for k in range(CONV - 1):
                total = total + pltpu.roll(raw, CONV - 1 - k, axis=0) * taps[k : k + 1]
            steps.append(step)
            logs.append(log)
            mixes.append(rounded(silu(total)))
        after = dot01(later, jnp.concatenate(logs, axis=1))
        for j in range(per):
            b = i * per + j
            after_here = after[:, j * LANES : (j + 1) * LANES]
            weight = jnp.exp(after_here) * steps[j]
            logs_ref[b : b + 1, :] = after_here[:1] + logs[j][:1]
            for k in range(CONV - 1):
                lead_weight_ref[k, b : b + 1, :] = weight[k : k + 1]
            weighted = jnp.where(position >= CONV - 1, mixes[j][:, :LANES] * weight, 0.0)
            state = dot(
                weighted.astype(BF16), mixes[j][:, LANES:].astype(BF16), ((0,), (0,))
            )
            state_ref[b] = state[:P_SIZE]
    trail_ref[...] = trail_f32[...].astype(BF16)


def token_body(
    x_ref, next_ref, value_ref, gate_ref, key_ref, query_ref, step_ref, qt_ref, bias_ref,
    decay_ref, skip_ref, trail_ref, taps_ref,
    out_map_ref, direct_ref, decay_out_ref, gate_out_ref,
    pad_ref, last_ref,
):
    prompts, block, width = x_ref.shape
    head = lax.axis_index(TP)
    group = head // (HEADS // GROUPS)
    at = pl.multiple_of(group * STATE, STATE)
    query = query_ref[:, pl.ds(at, STATE)]
    query_taps = qt_ref[:, pl.ds(at, STATE)].astype(F32)
    taps = taps_ref[...]
    last_ref[...] = rounded(dot(x_ref[...].reshape(prompts * block, width), query)).reshape(
        prompts, block, STATE
    )
    pad_ref[...] = jnp.zeros_like(pad_ref)
    pad_ref[:prompts] = next_ref[...].astype(F32)
    token = pad_ref[...].astype(BF16)
    new_value = rounded(dot(token, value_ref[...], ((1,), (1,))))
    new_key = rounded(dot(token, key_ref[:, pl.ds(at, STATE)]))
    new_query = rounded(dot(token, query))
    new_step = pick(rounded(dot(token, step_ref[...], ((1,), (1,)))), head)
    new_gate = rounded(dot(token, gate_ref[...], ((1,), (1,))))
    trail = trail_ref[...].astype(F32)
    value_sum = trail[0, :, :P_SIZE] * taps[:1, :P_SIZE]
    key_sum = trail[0, :, LANES:] * taps[:1, LANES:]
    query_sum = last_ref[:, block - 3, :] * query_taps[:1]
    for k in range(1, CONV - 1):
        value_sum = value_sum + trail[k, :, :P_SIZE] * taps[k : k + 1, :P_SIZE]
        key_sum = key_sum + trail[k, :, LANES:] * taps[k : k + 1, LANES:]
        query_sum = query_sum + last_ref[:, block - 3 + k, :] * query_taps[k : k + 1]
    new_input = rounded(silu(value_sum + new_value * taps[CONV - 1 : CONV, :P_SIZE]))
    new_in = rounded(silu(key_sum + new_key * taps[CONV - 1 : CONV, LANES:]))
    new_out = rounded(silu(query_sum + new_query[:prompts] * query_taps[CONV - 1 : CONV]))
    out_map_ref[...] = jnp.zeros_like(out_map_ref)
    out_map_ref[:prompts] = new_out
    step = softplus(new_step + pick(bias_ref[...], head))
    speed = jnp.exp(pick(decay_ref[...], head))
    decay_out_ref[...] = jnp.broadcast_to(jnp.exp(-speed * step), decay_out_ref.shape)
    agreement = jnp.sum(new_in * out_map_ref[...], axis=1, keepdims=True)
    direct_ref[...] = new_input * (step * agreement + pick(skip_ref[...], head))
    gate_out_ref[...] = silu(new_gate)


def pack_body(
    halo_ref, lead_ref, lead_weight_ref, logs_ref, taps_ref, state_ref, out_map_ref, direct_ref,
    out_ref,
):
    prompts, rows, _ = state_ref.shape
    dests = out_ref.shape[0]
    keep = rows // dests
    taps = taps_ref[...]
    window = [halo_ref[k].astype(F32) for k in range(CONV - 1)]
    window = window + [lead_ref[k] for k in range(CONV - 1)]
    weighted, maps = [], []
    for t in range(CONV - 1):
        total = window[t] * taps[:1]
        for k in range(1, CONV):
            total = total + window[t + k] * taps[k : k + 1]
        mixed = rounded(silu(total))
        weighted.append(jnp.transpose(rounded(mixed[:, :LANES] * lead_weight_ref[t])))
        maps.append(mixed[:, LANES:])
    states = []
    for b in range(prompts):
        state = state_ref[b]
        for t in range(CONV - 1):
            state = state + weighted[t][:rows, b : b + 1] * maps[t][b : b + 1]
        states.append(state)
    pair_rows = 2 * keep
    blocks = rows // pair_rows
    low = iota((blocks, pair_rows, STATE), 1) < keep
    for b in range(0, prompts, 2):
        one = states[b].reshape(blocks, pair_rows, STATE)
        two = states[b + 1].reshape(blocks, pair_rows, STATE)
        even = jnp.where(low, one, pltpu.roll(two, keep, axis=1))
        odd = jnp.where(low, pltpu.roll(one, keep, axis=1), two)
        at = b * keep
        for k in range(blocks):
            out_ref[2 * k, at : at + pair_rows, :] = even[k].astype(BF16)
            out_ref[2 * k + 1, at : at + pair_rows, :] = odd[k].astype(BF16)
    base = prompts * keep
    padded = out_map_ref.shape[0]
    direct = direct_ref[...]
    high = rounded(direct)
    low_part = direct - high
    log_parts = [part.astype(F32) for part in pieces(logs_ref[...])]
    lane = iota((padded, LANES), 1)
    log_lanes = jnp.where(
        lane == 2 * keep,
        log_parts[0],
        jnp.where(lane == 2 * keep + 1, log_parts[1], log_parts[2]),
    )
    new_out = out_map_ref[...].astype(BF16)
    wide = jnp.concatenate([high, low_part], axis=1)
    for d in range(dests):
        first = pltpu.roll(wide, (LANES - d * keep) % LANES, axis=1)
        second = pltpu.roll(wide, (LANES - P_SIZE - d * keep + keep) % LANES, axis=1)
        misc = jnp.where(lane < keep, first, jnp.where(lane < 2 * keep, second, log_lanes))
        out_ref[d, base : base + padded, :] = new_out
        out_ref[d, base + padded :, :] = misc.astype(BF16)


def read_body(
    parts_ref, decay_ref, gate_ref,
    cache_ref, gated_ref, squares_ref,
    *, prompts, keep,
):
    sources = parts_ref.shape[0]
    rows = prompts * keep
    padded = decay_ref.shape[0]
    shard = lax.axis_index("sp")
    repeat = (iota((rows, padded), 1) == iota((rows, padded), 0) // keep).astype(BF16)
    within = iota((rows, LANES), 0) % keep
    lane = iota((rows, LANES), 1)
    total = jnp.zeros((rows, STATE), F32)
    for s in range(sources):
        misc = dot(repeat, parts_ref[s, rows + padded :, :])
        log = jnp.sum(
            jnp.where((lane >= 2 * keep) & (lane < 2 * keep + 3), misc, 0.0), axis=1, keepdims=True
        )
        total = total * jnp.exp(log) + parts_ref[s, :rows, :].astype(F32)
    cache = total.astype(BF16)
    cache_ref[...] = cache
    new_out = dot(repeat, parts_ref[sources - 1, rows : rows + padded, :])
    read = jnp.sum(cache.astype(F32) * new_out, axis=1, keepdims=True)
    direct = jnp.sum(
        jnp.where((lane < 2 * keep) & (lane % keep == within), misc, 0.0), axis=1, keepdims=True
    )
    decay = dot01(repeat, decay_ref[...])
    gate = dot01(repeat, jnp.concatenate([gate_ref[...], gate_ref[...]], axis=1))
    gate = jnp.sum(jnp.where(lane == shard * keep + within, gate, 0.0), axis=1, keepdims=True)
    gated = (decay * read + direct) * gate
    spread = jnp.where(lane == iota((rows, LANES), 0) // keep, gated, 0.0)
    gather = (iota((8, rows), 0) == iota((8, rows), 1) % keep).astype(BF16)
    gated = dot01(gather, spread)
    gated_ref[...] = gated
    squares = jnp.sum(gated * gated, axis=0, keepdims=True)
    squares_ref[...] = jnp.broadcast_to(squares[None], squares_ref.shape)


def sum_body(parts_ref, out_ref):
    total = jnp.sum(parts_ref[...], axis=0, keepdims=True)
    out_ref[...] = jnp.broadcast_to(total, out_ref.shape)


def final_body(parts_ref, gated_ref, gain_ref, out_ref):
    _, keep, prompts = out_ref.shape
    heads, rows = gain_ref.shape
    head = lax.axis_index(TP)
    shard = lax.axis_index("sp")
    total = jnp.sum(parts_ref[...], axis=0)
    scale = lax.rsqrt(total / (heads * rows) + EPSILON)
    gain = jnp.broadcast_to(pick_row(gain_ref[...], head), (8, rows))
    own = iota((8, rows), 1) == shard * keep + iota((8, rows), 0)
    gain = jnp.sum(jnp.where(own, gain, 0.0), axis=1, keepdims=True)
    out = gated_ref[...] * scale * gain
    out_ref[0] = out[:keep, :prompts].astype(BF16)


def whole(count):
    return [pl.BlockSpec(memory_space=pltpu.VMEM) for _ in range(count)]


def call(body, outs, *operands, specs=None, scratch=(), name=None):
    return pl.pallas_call(
        body,
        in_specs=specs or whole(len(operands)),
        out_specs=whole(len(outs)),
        out_shape=outs,
        scratch_shapes=scratch,
        name=name,
    )(*operands)


def shards(
    prompt_layer_input,
    next_token_input,
    value_projection,
    output_gate_matrix,
    key_projection,
    query_projection,
    step_projection,
    value_filter_taps,
    key_filter_taps,
    query_filter_taps,
    step_size_bias,
    head_decay_logarithm,
    direct_path_weight,
    gated_norm_gain,
    position_decay_offset,
):
    prompts, length, width = prompt_layer_input.shape
    dests = lax.axis_size("sp")
    keep = P_SIZE // dests
    padded = -(-prompts // 8) * 8
    bias = step_size_bias[None]
    decay_rate = head_decay_logarithm[None]
    skip = direct_path_weight[None]
    out = jax.ShapeDtypeStruct
    value_rows = value_projection.T
    gate_rows = output_gate_matrix.T
    step_rows = step_projection.T
    offset_rows = jnp.swapaxes(position_decay_offset, 1, 2)

    per = 2
    state, trail, lead, lead_weight, logs, taps = call(
        lambda *refs: local_body(*refs, per=per),
        [
            out((prompts, P_SIZE, STATE), F32),
            out((CONV - 1, padded, 2 * LANES), BF16),
            out((CONV - 1, padded, 2 * LANES), F32),
            out((CONV - 1, padded, LANES), F32),
            out((padded, LANES), F32),
            out((8, 2 * LANES), F32),
        ],
        prompt_layer_input,
        value_rows,
        key_projection,
        step_rows,
        value_filter_taps,
        key_filter_taps,
        bias,
        decay_rate,
        offset_rows,
        specs=[pl.BlockSpec(memory_space=pl.ANY)] + whole(8),
        scratch=[
            pltpu.VMEM((prompts, length, width), BF16),
            pltpu.VMEM((width, 2 * LANES), BF16),
            pltpu.VMEM((CONV - 1, padded, 2 * LANES), F32),
            pltpu.SemaphoreType.DMA((prompts // per,)),
        ],
        name="local",
    )
    halo = lax.ppermute(trail, "sp", [(i, i + 1) for i in range(dests - 1)])
    block = 16
    token_operands = (
        prompt_layer_input,
        next_token_input,
        value_rows,
        gate_rows,
        key_projection,
        query_projection,
        step_rows,
        query_filter_taps,
        bias,
        decay_rate,
        skip,
        trail,
        taps,
    )
    tail = length // block - 1
    out_map, direct, new_decay, new_gate = pl.pallas_call(
        token_body,
        grid=(1,),
        in_specs=[pl.BlockSpec((prompts, block, width), lambda i: (0, tail, 0))]
        + whole(len(token_operands) - 1),
        out_specs=whole(4),
        out_shape=[
            out((padded, STATE), F32),
            out((padded, P_SIZE), F32),
            out((padded, LANES), F32),
            out((padded, P_SIZE), F32),
        ],
        scratch_shapes=[
            pltpu.VMEM((padded, width), F32),
            pltpu.VMEM((prompts, block, STATE), F32),
        ],
        name="token",
    )(*token_operands)
    (payload,) = call(
        pack_body,
        [out((dests, prompts * keep + 2 * padded, STATE), BF16)],
        halo,
        lead,
        lead_weight,
        logs,
        taps,
        state,
        out_map,
        direct,
        name="pack",
    )
    received = lax.all_to_all(payload, "sp", 0, 0, tiled=True)
    cache, gated, squares = call(
        lambda *refs: read_body(*refs, prompts=prompts, keep=keep),
        [
            out((prompts * keep, STATE), BF16),
            out((8, LANES), F32),
            out((dests, 1, LANES), F32),
        ],
        received,
        new_decay,
        new_gate,
        name="read",
    )
    squares = lax.all_to_all(squares, "sp", 0, 0, tiled=True)
    tp_size = lax.axis_size(TP)
    (squares,) = call(sum_body, [out((tp_size, 1, LANES), F32)], squares, name="sum")
    squares = lax.all_to_all(squares, TP, 0, 0, tiled=True)
    (first_read,) = call(
        final_body, [out((1, keep, prompts), BF16)], squares, gated, gated_norm_gain, name="final"
    )
    return cache.reshape(prompts, 1, keep, STATE), jnp.transpose(first_read, (2, 0, 1))


def solution(mesh):
    split = Mesh(
        mesh.devices.reshape(mesh.shape["grp"], mesh.shape["sp"], mesh.shape["tp"] // 2, 2),
        ("grp", "sp", "tp_0", "tp_1"),
    )
    return jax.shard_map(
        shards,
        mesh=split,
        in_specs=(
            P("grp", "sp", None),
            P("grp", None),
            P(None, TP),
            P(None, TP),
            P(),
            P(),
            P(),
            P(),
            P(),
            P(),
            P(),
            P(),
            P(),
            P(),
            P("grp", "sp", None),
        ),
        out_specs=(P("grp", TP, "sp", None), P("grp", TP, "sp")),
        check_vma=False,
    )
```

```python
import jax
import jax.numpy as jnp
from jax import lax
from jax.experimental import pallas as pl
from jax.experimental.pallas import tpu as pltpu
from jax.sharding import Mesh
from jax.sharding import PartitionSpec as P

HEADS = 32
P_SIZE = 64
GROUPS = 2
STATE = 128
CONV = 4
LANES = 128
TP = ("tp_0", "tp_1")
EPSILON = 1e-06

F32 = jnp.float32
BF16 = jnp.bfloat16


def rounded(value):
    return value.astype(BF16).astype(F32)


def silu(value):
    return value / (1.0 + jnp.exp(-value))


def softplus(value):
    return jnp.maximum(value, 0.0) + jnp.log1p(jnp.exp(-jnp.abs(value)))


def dot(a, b, dims=((1,), (0,))):
    return lax.dot_general(a, b, (dims, ((), ())), preferred_element_type=F32)


def pieces(value):
    first = value.astype(BF16)
    rest = value - first.astype(F32)
    second = rest.astype(BF16)
    third = (rest - second.astype(F32)).astype(BF16)
    return first, second, third


def dot01(matrix, value):
    a, b, c = pieces(value)
    return dot(jnp.concatenate([matrix] * 3, axis=1), jnp.concatenate([a, b, c], axis=0))


def iota(shape, dim):
    return lax.broadcasted_iota(jnp.int32, shape, dim)


def own_half(row, head):
    return jnp.where(head % 2 == 0, row, pltpu.roll(row, 64, axis=1))


def pick(row, lane):
    return jnp.sum(jnp.where(iota(row.shape, 1) == lane, row, 0.0), axis=1, keepdims=True)


def pick_row(matrix, row):
    matrix = matrix.astype(F32)
    return jnp.sum(jnp.where(iota(matrix.shape, 0) == row, matrix, 0.0), axis=0, keepdims=True)


def local_body(
    x_hbm, value_ref, key_ref, step_ref, vt_ref, kt_ref, bias_ref, decay_ref, off_ref,
    state_ref, lead_ref, lead_weight_ref, logs_ref, taps_ref,
    x_ref, w_ref, sems, *, per,
):
    prompts, length, width = x_hbm.shape
    copies = []
    for i in range(prompts // per):
        part = pl.ds(i * per, per)
        copies.append(pltpu.make_async_copy(x_hbm.at[part], x_ref.at[part], sems.at[i]))
    for copy in copies:
        copy.start()
    head = lax.axis_index(TP)
    group = head // (HEADS // GROUPS)
    step_row = jnp.broadcast_to(pick_row(step_ref[...], head), (P_SIZE, width)).astype(BF16)
    w_ref[:, :LANES] = jnp.transpose(jnp.concatenate([value_ref[...], step_row], axis=0))
    logs_ref[...] = jnp.zeros_like(logs_ref)
    at = pl.multiple_of(group * STATE, STATE)
    w_ref[:, LANES:] = key_ref[:, pl.ds(at, STATE)]
    pair = pl.multiple_of((head // 2) * LANES, LANES)
    value_taps = own_half(vt_ref[:, pl.ds(pair, LANES)].astype(F32), head)
    taps = jnp.concatenate([value_taps, kt_ref[:, pl.ds(at, STATE)].astype(F32)], axis=1)
    taps_ref[:CONV] = taps
    bias = pick(bias_ref[...], head)
    speed = jnp.exp(pick(decay_ref[...], head))
    later = (iota((length, length), 1) > iota((length, length), 0)).astype(BF16)
    position = iota((length, LANES), 0)
    for i in range(prompts // per):
        copies[i].wait()
        rows = x_ref[i * per : (i + 1) * per].reshape(per * length, width)
        raw_all = rounded(dot(rows, w_ref[...]))
        steps, logs, mixes = [], [], []
        for j in range(per):
            b = i * per + j
            raw = raw_all[j * length : (j + 1) * length]
            for k in range(CONV - 1):
                lead_ref[k, b : b + 1, :] = raw[k : k + 1]
            step = softplus(pltpu.roll(raw[:, :LANES], 64, axis=1) + bias)
            offset = jnp.broadcast_to(pick_row(off_ref[b], head), (length, length))
            log = jnp.transpose(offset) - speed * step
            total = raw * taps[CONV - 1 : CONV]
            for k in range(CONV - 1):
                total = total + pltpu.roll(raw, CONV - 1 - k, axis=0) * taps[k : k + 1]
            steps.append(step)
            logs.append(log)
            mixes.append(rounded(silu(total)))
        after = dot01(later, jnp.concatenate(logs, axis=1))
        for j in range(per):
            b = i * per + j
            after_here = after[:, j * LANES : (j + 1) * LANES]
            weight = jnp.exp(after_here) * steps[j]
            logs_ref[b : b + 1, :] = after_here[:1] + logs[j][:1]
            for k in range(CONV - 1):
                lead_weight_ref[k, b : b + 1, :] = weight[k : k + 1]
            weighted = jnp.where(position >= CONV - 1, mixes[j][:, :LANES] * weight, 0.0)
            state = dot(
                weighted.astype(BF16), mixes[j][:, LANES:].astype(BF16), ((0,), (0,))
            )
            state_ref[b] = state[:P_SIZE]


def token_body(
    x_ref, next_ref, value_ref, gate_ref, key_ref, query_ref, step_ref, vt_ref, kt_ref, qt_ref,
    bias_ref, decay_ref, skip_ref,
    trail_ref, newest_ref, decay_out_ref, gate_out_ref,
    pad_ref, last_ref,
):
    prompts, block, width = x_ref.shape
    head = lax.axis_index(TP)
    group = head // (HEADS // GROUPS)
    padded = pad_ref.shape[0]
    at = pl.multiple_of(group * STATE, STATE)
    pair = pl.multiple_of((head // 2) * LANES, LANES)
    query = query_ref[:, pl.ds(at, STATE)]
    key = key_ref[:, pl.ds(at, STATE)]
    value_taps = own_half(vt_ref[:, pl.ds(pair, LANES)].astype(F32), head)[:, :P_SIZE]
    key_taps = kt_ref[:, pl.ds(at, STATE)].astype(F32)
    query_taps = qt_ref[:, pl.ds(at, STATE)].astype(F32)
    pad_ref[...] = jnp.zeros_like(pad_ref)
    pad_ref[:prompts] = next_ref[...].astype(F32)
    token = pad_ref[...].astype(BF16)
    rows = jnp.concatenate([x_ref[...].reshape(prompts * block, width), token], axis=0)
    count = prompts * block
    values = rounded(dot(rows, value_ref[...], ((1,), (1,))))
    keys = rounded(dot(rows, key))
    queries = rounded(dot(rows, query))
    new_step = pick(rounded(dot(token, step_ref[...], ((1,), (1,)))), head)
    new_gate = rounded(dot(token, gate_ref[...], ((1,), (1,))))
    last_ref[...] = jnp.zeros_like(last_ref)
    for b in range(prompts):
        at_row = (b + 1) * block - (CONV - 1)
        for k in range(CONV - 1):
            row = slice(at_row + k, at_row + k + 1)
            last_ref[k, b : b + 1, :P_SIZE] = values[row]
            last_ref[k, b : b + 1, LANES : 2 * LANES] = keys[row]
            last_ref[k, b : b + 1, 2 * LANES :] = queries[row]
    last = last_ref[...]
    trail_ref[...] = last[:, :, : 2 * LANES].astype(BF16)
    value_sum = last[0, :, :P_SIZE] * value_taps[:1]
    key_sum = last[0, :, LANES : 2 * LANES] * key_taps[:1]
    query_sum = last[0, :, 2 * LANES :] * query_taps[:1]
    for k in range(1, CONV - 1):
        value_sum = value_sum + last[k, :, :P_SIZE] * value_taps[k : k + 1]
        key_sum = key_sum + last[k, :, LANES : 2 * LANES] * key_taps[k : k + 1]
        query_sum = query_sum + last[k, :, 2 * LANES :] * query_taps[k : k + 1]
    new_input = rounded(silu(value_sum + values[count:] * value_taps[CONV - 1 : CONV]))
    new_in = rounded(silu(key_sum + keys[count:] * key_taps[CONV - 1 : CONV]))
    new_out = rounded(silu(query_sum + queries[count:] * query_taps[CONV - 1 : CONV]))
    step = softplus(new_step + pick(bias_ref[...], head))
    speed = jnp.exp(pick(decay_ref[...], head))
    decay_out_ref[...] = jnp.broadcast_to(jnp.exp(-speed * step), decay_out_ref.shape)
    agreement = jnp.sum(new_in * new_out, axis=1, keepdims=True)
    direct = new_input * (step * agreement + pick(skip_ref[...], head))
    high = rounded(direct)
    direct = jnp.concatenate([high, direct - high], axis=1)
    newest = jnp.concatenate([new_out, direct], axis=0).astype(BF16)
    for d in range(newest_ref.shape[0]):
        newest_ref[d] = newest
    gate_out_ref[...] = silu(new_gate)


def pack_body(
    halo_ref, lead_ref, lead_weight_ref, logs_ref, taps_ref, state_ref, newest_ref, out_ref,
):
    prompts, rows, _ = state_ref.shape
    dests = out_ref.shape[0]
    keep = rows // dests
    padded = logs_ref.shape[0]
    taps = taps_ref[...]
    new_out = newest_ref[dests - 1, :padded, :].astype(F32)
    window = [halo_ref[k].astype(F32) for k in range(CONV - 1)]
    window = window + [lead_ref[k] for k in range(CONV - 1)]
    weighted, maps = [], []
    for t in range(CONV - 1):
        total = window[t] * taps[:1]
        for k in range(1, CONV):
            total = total + window[t + k] * taps[k : k + 1]
        mixed = rounded(silu(total))
        weighted.append(jnp.transpose(rounded(mixed[:, :LANES] * lead_weight_ref[t])))
        maps.append(mixed[:, LANES:])
    states = []
    reads = jnp.zeros((rows, LANES), F32)
    lane = iota((rows, LANES), 1)
    for b in range(prompts):
        state = state_ref[b]
        for t in range(CONV - 1):
            state = state + weighted[t][:rows, b : b + 1] * maps[t][b : b + 1]
        states.append(state)
        read = jnp.sum(state * new_out[b : b + 1], axis=1, keepdims=True)
        reads = jnp.where(lane == b, read, reads)
    pair_rows = 2 * keep
    blocks = rows // pair_rows
    low = iota((blocks, pair_rows, STATE), 1) < keep
    for b in range(0, prompts, 2):
        one = states[b].reshape(blocks, pair_rows, STATE)
        two = states[b + 1].reshape(blocks, pair_rows, STATE)
        even = jnp.where(low, one, pltpu.roll(two, keep, axis=1))
        odd = jnp.where(low, pltpu.roll(one, keep, axis=1), two)
        at = b * keep
        for k in range(blocks):
            out_ref[2 * k, at : at + pair_rows, :] = even[k].astype(BF16)
            out_ref[2 * k + 1, at : at + pair_rows, :] = odd[k].astype(BF16)
    reads = jnp.transpose(reads)[:padded]
    high = rounded(reads)
    extra = jnp.concatenate([high, reads - high], axis=1)
    corner = (padded, LANES)
    logs = jnp.where(iota(corner, 0) == iota(corner, 1), logs_ref[...], 0.0)
    logs = jnp.sum(logs, axis=0, keepdims=True)
    for k, part in enumerate(pieces(logs)):
        extra = jnp.where(iota(corner, 0) == prompts + k, part.astype(F32), extra)
    extra = extra.astype(BF16)
    for d in range(dests):
        out_ref[d, prompts * keep :, :] = extra


def read_body(
    parts_ref, newest_ref, decay_ref, gate_ref, cache_ref, gated_ref, squares_ref, *, prompts,
):
    sources, _, _ = parts_ref.shape
    padded = decay_ref.shape[0]
    rows = parts_ref.shape[1] - padded
    keep = rows // prompts
    shard = lax.axis_index("sp")
    state_own = iota((rows, LANES), 1) == iota((rows, LANES), 0) // keep
    read_own = iota((padded, LANES), 1) == iota((padded, LANES), 0)
    total = jnp.zeros((rows, STATE), F32)
    reads = jnp.zeros((padded, P_SIZE), F32)
    for s in range(sources):
        extra = parts_ref[s, rows:, :].astype(F32)
        decay = jnp.sum(extra[prompts : prompts + 3], axis=0, keepdims=True)
        decay = jnp.exp(decay)
        per_row = jnp.sum(jnp.where(state_own, decay, 0.0), axis=1, keepdims=True)
        per_prompt = jnp.sum(jnp.where(read_own, decay, 0.0), axis=1, keepdims=True)
        total = total * per_row + parts_ref[s, :rows, :].astype(F32)
        reads = reads * per_prompt + (extra[:, :P_SIZE] + extra[:, P_SIZE:])
    cache_ref[...] = total.astype(BF16)
    direct = newest_ref[sources - 1, padded:, :].astype(F32)
    direct = direct[:, :P_SIZE] + direct[:, P_SIZE:]
    gated = (decay_ref[:, :P_SIZE] * reads + direct) * gate_ref[...]
    gated = jnp.where(iota(gated.shape, 0) < prompts, gated, 0.0)
    squares = jnp.sum(gated * gated, axis=1, keepdims=True)
    squares = jnp.sum(jnp.where(read_own, squares, 0.0), axis=0, keepdims=True)
    squares_ref[...] = jnp.broadcast_to(squares[None], squares_ref.shape)
    square = jnp.concatenate([gated, jnp.zeros((P_SIZE - padded, P_SIZE), F32)], axis=0)
    square = jnp.concatenate([square, jnp.zeros((P_SIZE, P_SIZE), F32)], axis=0)
    square = jnp.concatenate([square, jnp.zeros((LANES, P_SIZE), F32)], axis=1)
    own = (iota((8, LANES), 1) == shard * keep + iota((8, LANES), 0)).astype(BF16)
    gated_ref[...] = dot01(own, jnp.transpose(square))


def final_body(parts_ref, gated_ref, gain_ref, out_ref):
    _, keep, prompts = out_ref.shape
    heads, rows = gain_ref.shape
    head = lax.axis_index(TP)
    shard = lax.axis_index("sp")
    total = jnp.sum(parts_ref[...], axis=0)
    scale = lax.rsqrt(total / (heads * rows) + EPSILON)
    gain = jnp.broadcast_to(pick_row(gain_ref[...], head), (8, rows))
    own = iota((8, rows), 1) == shard * keep + iota((8, rows), 0)
    gain = jnp.sum(jnp.where(own, gain, 0.0), axis=1, keepdims=True)
    out = gated_ref[...] * scale * gain
    out_ref[0] = out[:keep, :prompts].astype(BF16)


def whole(count):
    return [pl.BlockSpec(memory_space=pltpu.VMEM) for _ in range(count)]


def call(body, outs, *operands, specs=None, scratch=(), name=None):
    return pl.pallas_call(
        body,
        in_specs=specs or whole(len(operands)),
        out_specs=whole(len(outs)),
        out_shape=outs,
        scratch_shapes=scratch,
        name=name,
    )(*operands)


def shards(
    prompt_layer_input,
    next_token_input,
    value_projection,
    output_gate_matrix,
    key_projection,
    query_projection,
    step_projection,
    value_filter_taps,
    key_filter_taps,
    query_filter_taps,
    step_size_bias,
    head_decay_logarithm,
    direct_path_weight,
    gated_norm_gain,
    position_decay_offset,
):
    prompts, length, width = prompt_layer_input.shape
    dests = lax.axis_size("sp")
    keep = P_SIZE // dests
    padded = -(-prompts // 8) * 8
    bias = step_size_bias[None]
    decay_rate = head_decay_logarithm[None]
    skip = direct_path_weight[None]
    out = jax.ShapeDtypeStruct
    value_rows = value_projection.T
    gate_rows = output_gate_matrix.T
    step_rows = step_projection.T
    offset_rows = jnp.swapaxes(position_decay_offset, 1, 2)

    block = 16
    tail = length // block - 1
    token_operands = (
        prompt_layer_input,
        next_token_input,
        value_rows,
        gate_rows,
        key_projection,
        query_projection,
        step_rows,
        value_filter_taps,
        key_filter_taps,
        query_filter_taps,
        bias,
        decay_rate,
        skip,
    )
    trail, newest, new_decay, new_gate = pl.pallas_call(
        token_body,
        grid=(1,),
        in_specs=[pl.BlockSpec((prompts, block, width), lambda i: (0, tail, 0))]
        + whole(len(token_operands) - 1),
        out_specs=whole(4),
        out_shape=[
            out((CONV - 1, padded, 2 * LANES), BF16),
            out((dests, 2 * padded, LANES), BF16),
            out((padded, LANES), F32),
            out((padded, P_SIZE), F32),
        ],
        scratch_shapes=[
            pltpu.VMEM((padded, width), F32),
            pltpu.VMEM((CONV - 1, padded, 3 * LANES), F32),
        ],
        name="token",
    )(*token_operands)
    newest = lax.all_to_all(newest, "sp", 0, 0, tiled=True)
    halo = lax.ppermute(trail, "sp", [(i, i + 1) for i in range(dests - 1)])
    per = 2
    state, lead, lead_weight, logs, taps = call(
        lambda *refs: local_body(*refs, per=per),
        [
            out((prompts, P_SIZE, STATE), F32),
            out((CONV - 1, padded, 2 * LANES), F32),
            out((CONV - 1, padded, LANES), F32),
            out((padded, LANES), F32),
            out((8, 2 * LANES), F32),
        ],
        prompt_layer_input,
        value_rows,
        key_projection,
        step_rows,
        value_filter_taps,
        key_filter_taps,
        bias,
        decay_rate,
        offset_rows,
        specs=[pl.BlockSpec(memory_space=pl.ANY)] + whole(8),
        scratch=[
            pltpu.VMEM((prompts, length, width), BF16),
            pltpu.VMEM((width, 2 * LANES), BF16),
            pltpu.SemaphoreType.DMA((prompts // per,)),
        ],
        name="local",
    )
    (payload,) = call(
        pack_body,
        [out((dests, prompts * keep + padded, STATE), BF16)],
        halo,
        lead,
        lead_weight,
        logs,
        taps,
        state,
        newest,
        name="pack",
    )
    received = lax.all_to_all(payload, "sp", 0, 0, tiled=True)
    tp_size = lax.axis_size(TP)
    cache, gated, squares = call(
        lambda *refs: read_body(*refs, prompts=prompts),
        [
            out((prompts * keep, STATE), BF16),
            out((8, LANES), F32),
            out((tp_size, 1, LANES), F32),
        ],
        received,
        newest,
        new_decay,
        new_gate,
        name="read",
    )
    squares = lax.all_to_all(squares, TP, 0, 0, tiled=True)
    (first_read,) = call(
        final_body, [out((1, keep, prompts), BF16)], squares, gated, gated_norm_gain, name="final"
    )
    return cache.reshape(prompts, 1, keep, STATE), jnp.transpose(first_read, (2, 0, 1))


def solution(mesh):
    split = Mesh(
        mesh.devices.reshape(mesh.shape["grp"], mesh.shape["sp"], mesh.shape["tp"] // 2, 2),
        ("grp", "sp", "tp_0", "tp_1"),
    )
    return jax.shard_map(
        shards,
        mesh=split,
        in_specs=(
            P("grp", "sp", None),
            P("grp", None),
            P(None, TP),
            P(None, TP),
            P(),
            P(),
            P(),
            P(),
            P(),
            P(),
            P(),
            P(),
            P(),
            P(),
            P("grp", "sp", None),
        ),
        out_specs=(P("grp", TP, "sp", None), P("grp", TP, "sp")),
        check_vma=False,
    )
```

```python
import jax
import jax.numpy as jnp
from jax import lax
from jax.experimental import pallas as pl
from jax.experimental.pallas import tpu as pltpu
from jax.sharding import Mesh
from jax.sharding import PartitionSpec as P

HEADS = 32
P_SIZE = 64
GROUPS = 2
STATE = 128
CONV = 4
LANES = 128
TP = ("tp_0", "tp_1")
EPSILON = 1e-06

F32 = jnp.float32
BF16 = jnp.bfloat16


def rounded(value):
    return value.astype(BF16).astype(F32)


def silu(value):
    return value / (1.0 + jnp.exp(-value))


def softplus(value):
    return jnp.maximum(value, 0.0) + jnp.log1p(jnp.exp(-jnp.abs(value)))


def dot(a, b, dims=((1,), (0,))):
    return lax.dot_general(a, b, (dims, ((), ())), preferred_element_type=F32)


def pieces(value):
    first = value.astype(BF16)
    rest = value - first.astype(F32)
    second = rest.astype(BF16)
    third = (rest - second.astype(F32)).astype(BF16)
    return first, second, third


def dot01(matrix, value):
    a, b, c = pieces(value)
    return dot(jnp.concatenate([matrix] * 3, axis=1), jnp.concatenate([a, b, c], axis=0))


def iota(shape, dim):
    return lax.broadcasted_iota(jnp.int32, shape, dim)


def own_half(row, head):
    return jnp.where(head % 2 == 0, row, pltpu.roll(row, 64, axis=1))


def pick(row, lane):
    return jnp.sum(jnp.where(iota(row.shape, 1) == lane, row, 0.0), axis=1, keepdims=True)


def pick_row(matrix, row):
    matrix = matrix.astype(F32)
    return jnp.sum(jnp.where(iota(matrix.shape, 0) == row, matrix, 0.0), axis=0, keepdims=True)


def local_body(
    x_hbm, value_ref, key_ref, step_ref, vt_ref, kt_ref, bias_ref, decay_ref, off_ref,
    state_ref, lead_ref, lead_weight_ref, logs_ref, taps_ref,
    x_ref, w_ref, sems, *, per,
):
    prompts, length, width = x_hbm.shape
    copies = []
    for i in range(prompts // per):
        part = pl.ds(i * per, per)
        copies.append(pltpu.make_async_copy(x_hbm.at[part], x_ref.at[part], sems.at[i]))
    for copy in copies:
        copy.start()
    head = lax.axis_index(TP)
    group = head // (HEADS // GROUPS)
    step_row = jnp.broadcast_to(pick_row(step_ref[...], head), (P_SIZE, width)).astype(BF16)
    w_ref[:, :LANES] = jnp.transpose(jnp.concatenate([value_ref[...], step_row], axis=0))
    logs_ref[...] = jnp.zeros_like(logs_ref)
    at = pl.multiple_of(group * STATE, STATE)
    w_ref[:, LANES:] = key_ref[:, pl.ds(at, STATE)]
    pair = pl.multiple_of((head // 2) * LANES, LANES)
    value_taps = own_half(vt_ref[:, pl.ds(pair, LANES)].astype(F32), head)
    taps = jnp.concatenate([value_taps, kt_ref[:, pl.ds(at, STATE)].astype(F32)], axis=1)
    taps_ref[:CONV] = taps
    bias = pick(bias_ref[...], head)
    speed = jnp.exp(pick(decay_ref[...], head))
    later = (iota((length, length), 1) > iota((length, length), 0)).astype(BF16)
    position = iota((length, LANES), 0)
    for i in range(prompts // per):
        copies[i].wait()
        rows = x_ref[i * per : (i + 1) * per].reshape(per * length, width)
        raw_all = rounded(dot(rows, w_ref[...]))
        steps, logs, mixes = [], [], []
        for j in range(per):
            b = i * per + j
            raw = raw_all[j * length : (j + 1) * length]
            for k in range(CONV - 1):
                lead_ref[k, b : b + 1, :] = raw[k : k + 1]
            step = softplus(pltpu.roll(raw[:, :LANES], 64, axis=1) + bias)
            offset = jnp.broadcast_to(pick_row(off_ref[b], head), (length, length))
            log = jnp.transpose(offset) - speed * step
            total = raw * taps[CONV - 1 : CONV]
            for k in range(CONV - 1):
                total = total + pltpu.roll(raw, CONV - 1 - k, axis=0) * taps[k : k + 1]
            steps.append(step)
            logs.append(log)
            mixes.append(rounded(silu(total)))
        after = dot01(later, jnp.concatenate(logs, axis=1))
        for j in range(per):
            b = i * per + j
            after_here = after[:, j * LANES : (j + 1) * LANES]
            weight = jnp.exp(after_here) * steps[j]
            logs_ref[b : b + 1, :] = after_here[:1] + logs[j][:1]
            for k in range(CONV - 1):
                lead_weight_ref[k, b : b + 1, :] = weight[k : k + 1]
            weighted = jnp.where(position >= CONV - 1, mixes[j][:, :LANES] * weight, 0.0)
            state = dot(
                weighted.astype(BF16), mixes[j][:, LANES:].astype(BF16), ((0,), (0,))
            )
            state_ref[b] = state[:P_SIZE]


def token_body(
    x_ref, next_ref, value_ref, gate_ref, key_ref, query_ref, step_ref, vt_ref, kt_ref, qt_ref,
    bias_ref, decay_ref, skip_ref,
    trail_ref, newest_ref, decay_out_ref, gate_out_ref,
    pad_ref, last_ref,
):
    prompts, block, width = x_ref.shape
    head = lax.axis_index(TP)
    group = head // (HEADS // GROUPS)
    at = pl.multiple_of(group * STATE, STATE)
    pair = pl.multiple_of((head // 2) * LANES, LANES)
    query = query_ref[:, pl.ds(at, STATE)]
    key = key_ref[:, pl.ds(at, STATE)]
    value_taps = own_half(vt_ref[:, pl.ds(pair, LANES)].astype(F32), head)[:, :P_SIZE]
    key_taps = kt_ref[:, pl.ds(at, STATE)].astype(F32)
    query_taps = qt_ref[:, pl.ds(at, STATE)].astype(F32)
    pad_ref[...] = jnp.zeros_like(pad_ref)
    pad_ref[:prompts] = next_ref[...].astype(F32)
    token = pad_ref[...].astype(BF16)
    rows = jnp.concatenate([x_ref[...].reshape(prompts * block, width), token], axis=0)
    count = prompts * block
    values = rounded(dot(rows, value_ref[...], ((1,), (1,))))
    keys = rounded(dot(rows, key))
    queries = rounded(dot(rows, query))
    new_step = pick(rounded(dot(token, step_ref[...], ((1,), (1,)))), head)
    new_gate = rounded(dot(token, gate_ref[...], ((1,), (1,))))
    last_ref[...] = jnp.zeros_like(last_ref)
    for b in range(prompts):
        at_row = (b + 1) * block - (CONV - 1)
        for k in range(CONV - 1):
            row = slice(at_row + k, at_row + k + 1)
            last_ref[k, b : b + 1, :P_SIZE] = values[row]
            last_ref[k, b : b + 1, LANES : 2 * LANES] = keys[row]
            last_ref[k, b : b + 1, 2 * LANES :] = queries[row]
    last = last_ref[...]
    trail_ref[...] = last[:, :, : 2 * LANES].astype(BF16)
    value_sum = last[0, :, :P_SIZE] * value_taps[:1]
    key_sum = last[0, :, LANES : 2 * LANES] * key_taps[:1]
    query_sum = last[0, :, 2 * LANES :] * query_taps[:1]
    for k in range(1, CONV - 1):
        value_sum = value_sum + last[k, :, :P_SIZE] * value_taps[k : k + 1]
        key_sum = key_sum + last[k, :, LANES : 2 * LANES] * key_taps[k : k + 1]
        query_sum = query_sum + last[k, :, 2 * LANES :] * query_taps[k : k + 1]
    new_input = rounded(silu(value_sum + values[count:] * value_taps[CONV - 1 : CONV]))
    new_in = rounded(silu(key_sum + keys[count:] * key_taps[CONV - 1 : CONV]))
    new_out = rounded(silu(query_sum + queries[count:] * query_taps[CONV - 1 : CONV]))
    step = softplus(new_step + pick(bias_ref[...], head))
    speed = jnp.exp(pick(decay_ref[...], head))
    decay_out_ref[...] = jnp.broadcast_to(jnp.exp(-speed * step), decay_out_ref.shape)
    agreement = jnp.sum(new_in * new_out, axis=1, keepdims=True)
    direct = new_input * (step * agreement + pick(skip_ref[...], head))
    high = rounded(direct)
    direct = jnp.concatenate([high, direct - high], axis=1)
    newest_ref[...] = jnp.concatenate([new_out, direct], axis=0).astype(BF16)
    gate_out_ref[...] = silu(new_gate)


def pack_body(
    halo_ref, lead_ref, lead_weight_ref, logs_ref, taps_ref, state_ref, newest_ref, out_ref,
):
    prompts, rows, _ = state_ref.shape
    padded = logs_ref.shape[0]
    taps = taps_ref[...]
    window = [halo_ref[k].astype(F32) for k in range(CONV - 1)]
    window = window + [lead_ref[k] for k in range(CONV - 1)]
    weighted, maps = [], []
    for t in range(CONV - 1):
        total = window[t] * taps[:1]
        for k in range(1, CONV):
            total = total + window[t + k] * taps[k : k + 1]
        mixed = rounded(silu(total))
        weighted.append(jnp.transpose(rounded(mixed[:, :LANES] * lead_weight_ref[t])))
        maps.append(mixed[:, LANES:])
    for b in range(prompts):
        state = state_ref[b]
        for t in range(CONV - 1):
            state = state + weighted[t][:rows, b : b + 1] * maps[t][b : b + 1]
        out_ref[b * rows : (b + 1) * rows] = state.astype(BF16)
    base = prompts * rows
    logs = jnp.zeros((padded, LANES), F32)
    for k, part in enumerate(pieces(logs_ref[...])):
        logs = jnp.where(iota(logs.shape, 1) == k, part.astype(F32), logs)
    out_ref[base : base + padded] = logs.astype(BF16)
    out_ref[base + padded :] = newest_ref[...]


def log_of(part_ref, base, padded):
    log = jnp.sum(part_ref[base : base + padded].astype(F32), axis=1, keepdims=True)
    return jnp.broadcast_to(log, (padded, LANES))


def followed(states, part_ref, log):
    decay = jnp.exp(log)
    rows = states[0].shape[0]
    return [
        state * decay[b : b + 1] + part_ref[b * rows : (b + 1) * rows].astype(F32)
        for b, state in enumerate(states)
    ]


def joined_shards(refs, base, padded, prompts):
    rows = base // prompts
    states = [refs[0][b * rows : (b + 1) * rows].astype(F32) for b in range(prompts)]
    logs = log_of(refs[0], base, padded)
    for ref in refs[1:]:
        log = log_of(ref, base, padded)
        logs = logs + log
        states = followed(states, ref, log)
    return states, logs


def early_body(*refs, prompts, padded, half):
    parts, (one_ref, two_ref, logs_ref, newest_ref) = refs[:-4], refs[-4:]
    base = prompts * P_SIZE
    one, one_log = joined_shards(parts[:half], base, padded, prompts)
    two, two_log = joined_shards(parts[half:], base, padded, prompts)
    for b in range(prompts):
        one_ref[b] = one[b]
        two_ref[b] = two[b]
    logs_ref[0] = one_log
    logs_ref[1] = two_log
    newest_ref[...] = parts[half - 1][base + padded :]


def hub_body(
    one_ref, two_ref, logs_ref, newest_ref, before_ref, last_ref, decay_ref, gate_ref,
    own_ref, next_ref, pair_ref, rest_ref, *, half, keep,
):
    prompts, rows, _ = one_ref.shape
    padded = decay_ref.shape[0]
    base = prompts * rows
    low = lax.axis_index("sp") < half
    two_log = logs_ref[1]
    two = [two_ref[b] for b in range(prompts)]
    for ref in (before_ref, last_ref):
        log = log_of(ref, base, padded)
        two_log = two_log + log
        two = followed(two, ref, log)
    one_decay = jnp.exp(jnp.where(low, two_log, 0.0))
    two_decay = jnp.exp(jnp.where(low, 0.0, logs_ref[0]))
    newest = jnp.where(
        low, last_ref[base + padded :].astype(F32), newest_ref[...].astype(F32)
    )
    new_out = newest[:padded]
    lane = iota((rows, LANES), 1)
    reads = jnp.zeros((rows, LANES), F32)
    kept = []
    for b in range(prompts):
        state = rounded(one_ref[b] * one_decay[b : b + 1] + two[b] * two_decay[b : b + 1])
        read = jnp.sum(state * new_out[b : b + 1], axis=1, keepdims=True)
        reads = jnp.where(lane == b, read, reads)
        kept.append(jnp.where(low, state[: rows // 2], state[rows // 2 :]))
    corner = (padded, LANES)
    decay = jnp.where(iota(corner, 0) == iota(corner, 1), decay_ref[...], 0.0)
    decay = jnp.sum(decay, axis=0, keepdims=True)
    below = jnp.zeros((LANES - padded, LANES), F32)
    direct = jnp.transpose(jnp.concatenate([newest[padded:], below], axis=0))
    direct = direct[:rows] + direct[rows:]
    gate = jnp.concatenate([gate_ref[...], gate_ref[...]], axis=1)
    gate = jnp.transpose(jnp.concatenate([gate, below], axis=0))[:rows]
    gated = jnp.where(lane < prompts, (decay * reads + direct) * gate, 0.0)
    squares = jnp.sum(gated * gated, axis=0, keepdims=True)
    gated = jnp.where(low, gated[: rows // 2], gated[rows // 2 :])
    count = rows // 2
    square_rows = jnp.zeros(corner, F32)
    for k, part in enumerate(pieces(squares)):
        square_rows = jnp.where(iota(corner, 0) == k, part.astype(F32), square_rows)
    stack = jnp.concatenate([*pieces(gated), square_rows.astype(BF16)], axis=0)
    chosen = (16 * half, stack.shape[0])
    dest, at, col = iota(chosen, 0) // 16, iota(chosen, 0) % 16, iota(chosen, 1)
    source = jnp.where(
        at < 3 * keep,
        (at // keep) * count + dest * keep + at % keep,
        3 * count + at - 3 * keep,
    )
    extra = dot((col == source).astype(BF16), stack).astype(BF16)

    def place(dest):
        if dest == 0:
            return own_ref, 0
        if dest == 1:
            return next_ref, 0
        return (pair_ref, dest - 2) if dest < 4 else (rest_ref, dest - 4)

    pair_rows = 2 * keep
    blocks = count // pair_rows
    first = iota((blocks, pair_rows, STATE), 1) < keep
    for b in range(0, prompts, 2):
        one = kept[b].reshape(blocks, pair_rows, STATE)
        two = kept[b + 1].reshape(blocks, pair_rows, STATE)
        even = jnp.where(first, one, pltpu.roll(two, keep, axis=1)).astype(BF16)
        odd = jnp.where(first, pltpu.roll(one, keep, axis=1), two).astype(BF16)
        for k in range(blocks):
            for dest, value in ((2 * k, even[k]), (2 * k + 1, odd[k])):
                ref, i = place(dest)
                ref[i, b * keep : (b + 2) * keep, :] = value
    for d in range(half):
        ref, i = place(d)
        ref[i, prompts * keep :, :] = extra[d * 16 : (d + 1) * 16]


def pick_body(
    own_ref, next_ref, pair_ref, rest_ref, sixth_ref, odd_ref,
    cache_ref, gated_ref, squares_ref, *, half, keep,
):
    rows = cache_ref.shape[0]
    at_hub = lax.axis_index("sp") % half == 0
    mine = jnp.where(at_hub, own_ref[0].astype(F32), 0.0)
    for value in (next_ref[0], pair_ref[0], rest_ref[0], sixth_ref[2], odd_ref[0]):
        mine = mine + value.astype(F32)
    mine = mine.astype(BF16)
    cache_ref[...] = mine[:rows]
    shape = (8, 16)
    row, col = iota(shape, 0), iota(shape, 1)
    chosen = ((row < keep) & (col < 3 * keep) & (col % keep == row)) | (
        (row == keep) & (col >= 3 * keep) & (col < 3 * keep + 3)
    )
    values = dot(chosen.astype(BF16), mine[rows:])
    gated_ref[...] = values
    squares_ref[...] = jnp.broadcast_to(values[keep : keep + 1][None], squares_ref.shape)


def final_body(parts_ref, gated_ref, gain_ref, out_ref):
    _, keep, prompts = out_ref.shape
    heads, rows = gain_ref.shape
    head = lax.axis_index(TP)
    shard = lax.axis_index("sp")
    total = jnp.sum(parts_ref[...], axis=0)
    scale = lax.rsqrt(total / (heads * rows) + EPSILON)
    gain = jnp.broadcast_to(pick_row(gain_ref[...], head), (8, rows))
    own = iota((8, rows), 1) == shard * keep + iota((8, rows), 0)
    gain = jnp.sum(jnp.where(own, gain, 0.0), axis=1, keepdims=True)
    out = gated_ref[...] * scale * gain
    out_ref[0] = out[:keep, :prompts].astype(BF16)


def whole(count):
    return [pl.BlockSpec(memory_space=pltpu.VMEM) for _ in range(count)]


def call(body, outs, *operands, specs=None, scratch=()):
    return pl.pallas_call(
        body,
        in_specs=specs or whole(len(operands)),
        out_specs=whole(len(outs)),
        out_shape=outs,
        scratch_shapes=scratch,
    )(*operands)


def shards(
    prompt_layer_input,
    next_token_input,
    value_projection,
    output_gate_matrix,
    key_projection,
    query_projection,
    step_projection,
    value_filter_taps,
    key_filter_taps,
    query_filter_taps,
    step_size_bias,
    head_decay_logarithm,
    direct_path_weight,
    gated_norm_gain,
    position_decay_offset,
):
    prompts, length, width = prompt_layer_input.shape
    dests = lax.axis_size("sp")
    keep = P_SIZE // dests
    padded = -(-prompts // 8) * 8
    bias = step_size_bias[None]
    decay_rate = head_decay_logarithm[None]
    skip = direct_path_weight[None]
    out = jax.ShapeDtypeStruct
    value_rows = value_projection.T
    gate_rows = output_gate_matrix.T
    step_rows = step_projection.T
    offset_rows = jnp.swapaxes(position_decay_offset, 1, 2)

    block = 16
    tail = length // block - 1
    token_operands = (
        prompt_layer_input,
        next_token_input,
        value_rows,
        gate_rows,
        key_projection,
        query_projection,
        step_rows,
        value_filter_taps,
        key_filter_taps,
        query_filter_taps,
        bias,
        decay_rate,
        skip,
    )
    trail, newest, new_decay, new_gate = pl.pallas_call(
        token_body,
        grid=(1,),
        in_specs=[pl.BlockSpec((prompts, block, width), lambda i: (0, tail, 0))]
        + whole(len(token_operands) - 1),
        out_specs=whole(4),
        out_shape=[
            out((CONV - 1, padded, 2 * LANES), BF16),
            out((2 * padded, LANES), BF16),
            out((padded, LANES), F32),
            out((padded, P_SIZE), F32),
        ],
        scratch_shapes=[
            pltpu.VMEM((padded, width), F32),
            pltpu.VMEM((CONV - 1, padded, 3 * LANES), F32),
        ],
        name="token",
    )(*token_operands)
    halo = lax.ppermute(trail, "sp", [(i, i + 1) for i in range(dests - 1)])
    per = 2
    state, lead, lead_weight, logs, taps = call(
        lambda *refs: local_body(*refs, per=per),
        [
            out((prompts, P_SIZE, STATE), F32),
            out((CONV - 1, padded, 2 * LANES), F32),
            out((CONV - 1, padded, LANES), F32),
            out((padded, LANES), F32),
            out((8, 2 * LANES), F32),
        ],
        prompt_layer_input,
        value_rows,
        key_projection,
        step_rows,
        value_filter_taps,
        key_filter_taps,
        bias,
        decay_rate,
        offset_rows,
        specs=[pl.BlockSpec(memory_space=pl.ANY)] + whole(8),
        scratch=[
            pltpu.VMEM((prompts, length, width), BF16),
            pltpu.VMEM((width, 2 * LANES), BF16),
            pltpu.SemaphoreType.DMA((prompts // per,)),
        ],
    )
    (payload,) = call(
        pack_body,
        [out((prompts * P_SIZE + 3 * padded, STATE), BF16)],
        halo,
        lead,
        lead_weight,
        logs,
        taps,
        state,
        newest,
    )
    half = dests // 2
    parts = {0: payload}
    for k in range(dests - 1, 0, -1):
        pairs = [(k, 0), ((half + k) % dests, half)]
        parts[k] = lax.ppermute(payload, "sp", pairs)
    states = out((prompts, P_SIZE, STATE), F32)
    one, two, early_logs, early_newest = call(
        lambda *refs: early_body(*refs, prompts=prompts, padded=padded, half=half),
        [states, states, out((2, padded, LANES), F32), out((2 * padded, LANES), BF16)],
        *[parts[k] for k in range(dests - 2)],
    )
    entry = prompts * keep + 16
    own, to_next, to_pair, to_rest = call(
        lambda *refs: hub_body(*refs, half=half, keep=keep),
        [out((n, entry, STATE), BF16) for n in (1, 1, 2, 4)],
        one,
        two,
        early_logs,
        early_newest,
        parts[dests - 2],
        parts[dests - 1],
        new_decay,
        new_gate,
    )

    def hop(value, *moves):
        pairs = [(h + i, h + j) for h in (0, half) for i, j in moves]
        return lax.ppermute(value, "sp", pairs)

    to_next = hop(to_next, (0, 1))
    to_pair = hop(to_pair, (0, 2))
    to_rest = hop(to_rest, (0, 4))
    to_sixth = hop(to_rest, (4, 6))
    to_odd = hop(to_pair[1:] + to_rest[1:2] + to_sixth[3:], (2, 3), (4, 5), (6, 7))
    tp_size = lax.axis_size(TP)
    cache, gated, squares = call(
        lambda *refs: pick_body(*refs, half=half, keep=keep),
        [
            out((prompts * keep, STATE), BF16),
            out((8, LANES), F32),
            out((tp_size, 1, LANES), F32),
        ],
        own,
        to_next,
        to_pair,
        to_rest,
        to_sixth,
        to_odd,
    )
    squares = lax.all_to_all(squares, TP, 0, 0, tiled=True)
    (first_read,) = call(
        final_body, [out((1, keep, prompts), BF16)], squares, gated, gated_norm_gain
    )
    return cache.reshape(prompts, 1, keep, STATE), jnp.transpose(first_read, (2, 0, 1))


def solution(mesh):
    split = Mesh(
        mesh.devices.reshape(mesh.shape["grp"], mesh.shape["sp"], mesh.shape["tp"] // 2, 2),
        ("grp", "sp", "tp_0", "tp_1"),
    )
    return jax.shard_map(
        shards,
        mesh=split,
        in_specs=(
            P("grp", "sp", None),
            P("grp", None),
            P(None, TP),
            P(None, TP),
            P(),
            P(),
            P(),
            P(),
            P(),
            P(),
            P(),
            P(),
            P(),
            P(),
            P("grp", "sp", None),
        ),
        out_specs=(P("grp", TP, "sp", None), P("grp", TP, "sp")),
        check_vma=False,
    )
```

```python
import jax
import jax.numpy as jnp
from jax import lax
from jax.experimental import pallas as pl
from jax.experimental.pallas import tpu as pltpu
from jax.sharding import Mesh
from jax.sharding import PartitionSpec as P

HEADS = 32
P_SIZE = 64
GROUPS = 2
STATE = 128
CONV = 4
LANES = 128
TP = ("tp_0", "tp_1")
EPSILON = 1e-06

F32 = jnp.float32
BF16 = jnp.bfloat16


def rounded(value):
    return value.astype(BF16).astype(F32)


def silu(value):
    return value / (1.0 + jnp.exp(-value))


def softplus(value):
    return jnp.maximum(value, 0.0) + jnp.log1p(jnp.exp(-jnp.abs(value)))


def dot(a, b, dims=((1,), (0,))):
    return lax.dot_general(a, b, (dims, ((), ())), preferred_element_type=F32)


def pieces(value):
    first = value.astype(BF16)
    rest = value - first.astype(F32)
    second = rest.astype(BF16)
    third = (rest - second.astype(F32)).astype(BF16)
    return first, second, third


def iota(shape, dim):
    return lax.broadcasted_iota(jnp.int32, shape, dim)


def own_half(row, head):
    return jnp.where(head % 2 == 0, row, pltpu.roll(row, 64, axis=1))


def pick(row, lane):
    return jnp.sum(jnp.where(iota(row.shape, 1) == lane, row, 0.0), axis=1, keepdims=True)


def pick_row(matrix, row):
    matrix = matrix.astype(F32)
    return jnp.sum(jnp.where(iota(matrix.shape, 0) == row, matrix, 0.0), axis=0, keepdims=True)


def local_body(
    x_hbm, key_hbm, value_ref, step_ref, vt_ref, kt_ref, bias_ref, decay_ref, off_ref,
    state_ref, lead_ref, weight_ref, logs_ref, taps_ref,
    x_ref, w_ref, wide_ref, map_ref, rows_ref, key_sem, sems, *, per,
):
    prompts, length, width = x_hbm.shape
    head = lax.axis_index(TP)
    group = head // (HEADS // GROUPS)
    at = pl.multiple_of(group * STATE, STATE)
    key_copy = pltpu.make_async_copy(
        key_hbm.at[:, pl.ds(at, STATE)], w_ref.at[:, pl.ds(LANES, STATE)], key_sem
    )
    key_copy.start()
    copies = []
    for i in range(prompts // per):
        part = pl.ds(i * per, per)
        copies.append(pltpu.make_async_copy(x_hbm.at[part], x_ref.at[part], sems.at[i]))
    for copy in copies:
        copy.start()
    step_row = jnp.broadcast_to(pick_row(step_ref[...], head), (P_SIZE, width)).astype(BF16)
    w_ref[:, :LANES] = jnp.transpose(jnp.concatenate([value_ref[...], step_row], axis=0))
    pair = pl.multiple_of((head // 2) * LANES, LANES)
    value_taps = own_half(vt_ref[:, pl.ds(pair, LANES)].astype(F32), head)
    taps = jnp.concatenate([value_taps, kt_ref[:, pl.ds(at, STATE)].astype(F32)], axis=1)
    taps_ref[:CONV] = taps
    rows_ref[...] = jnp.zeros_like(rows_ref)
    offset = off_ref[...]
    offset = jnp.where(iota(offset.shape, 1) == head, offset, 0.0)
    rows_ref[1, :prompts] = jnp.sum(offset, axis=1)
    feature = iota((length, LANES), 1) < P_SIZE
    key_copy.wait()
    for i in range(prompts // per):
        copies[i].wait()
        rows = x_ref[i * per : (i + 1) * per].reshape(per * length, width)
        raw_all = rounded(dot(rows, w_ref[...]))
        for j in range(per):
            b = i * per + j
            raw = raw_all[j * length : (j + 1) * length]
            for k in range(CONV - 1):
                lead_ref[k, b : b + 1, :] = raw[k : k + 1]
            total = raw * taps[CONV - 1 : CONV]
            for k in range(CONV - 1):
                total = total + pltpu.roll(raw, CONV - 1 - k, axis=0) * taps[k : k + 1]
            mixed = silu(total)
            map_ref[b] = mixed[:, LANES:].astype(BF16)
            turned = jnp.where(feature, rounded(mixed[:, :LANES]), raw[:, :LANES])
            turned = jnp.transpose(turned)
            wide_ref[b] = turned[:P_SIZE]
            rows_ref[0, b : b + 1, :] = turned[P_SIZE : P_SIZE + 1]
    step = softplus(rows_ref[0] + pick(bias_ref[...], head))
    log = rows_ref[1] - jnp.exp(pick(decay_ref[...], head)) * step
    later = (iota((length, length), 0) > iota((length, length), 1)).astype(BF16)
    after = dot(jnp.concatenate(pieces(log), axis=1), jnp.concatenate([later] * 3, axis=0))
    weight = jnp.exp(after) * step
    weight_ref[...] = weight
    logs_ref[...] = jnp.broadcast_to(jnp.sum(log, axis=1, keepdims=True), logs_ref.shape)
    weight = jnp.where(iota(weight.shape, 1) >= CONV - 1, weight, 0.0)
    for b in range(prompts):
        weighted = (wide_ref[b] * weight[b : b + 1]).astype(BF16)
        state_ref[b] = dot(weighted, map_ref[b])


def token_body(
    key_hbm, query_hbm, x_ref, next_ref, value_ref, gate_ref, step_ref, vt_ref, kt_ref, qt_ref,
    bias_ref, decay_ref, skip_ref,
    trail_ref, newest_ref, decay_out_ref, gate_out_ref,
    pad_ref, last_ref, key_ref, query_ref, sems,
):
    prompts, block, width = x_ref.shape
    head = lax.axis_index(TP)
    group = head // (HEADS // GROUPS)
    at = pl.multiple_of(group * STATE, STATE)
    pair = pl.multiple_of((head // 2) * LANES, LANES)
    copies = [
        pltpu.make_async_copy(source.at[:, pl.ds(at, STATE)], target, sems.at[i])
        for i, (source, target) in enumerate(((key_hbm, key_ref), (query_hbm, query_ref)))
    ]
    for copy in copies:
        copy.start()
    value_taps = own_half(vt_ref[:, pl.ds(pair, LANES)].astype(F32), head)[:, :P_SIZE]
    key_taps = kt_ref[:, pl.ds(at, STATE)].astype(F32)
    query_taps = qt_ref[:, pl.ds(at, STATE)].astype(F32)
    pad_ref[...] = jnp.zeros_like(pad_ref)
    pad_ref[:prompts] = next_ref[...].astype(F32)
    token = pad_ref[...].astype(BF16)
    rows = jnp.concatenate([x_ref[...].reshape(prompts * block, width), token], axis=0)
    count = prompts * block
    values = rounded(dot(rows, value_ref[...], ((1,), (1,))))
    new_step = pick(rounded(dot(token, step_ref[...], ((1,), (1,)))), head)
    new_gate = rounded(dot(token, gate_ref[...], ((1,), (1,))))
    copies[0].wait()
    keys = rounded(dot(rows, key_ref[...]))
    copies[1].wait()
    queries = rounded(dot(rows, query_ref[...]))
    last_ref[...] = jnp.zeros_like(last_ref)
    for b in range(prompts):
        at_row = (b + 1) * block - (CONV - 1)
        for k in range(CONV - 1):
            row = slice(at_row + k, at_row + k + 1)
            last_ref[k, b : b + 1, :P_SIZE] = values[row]
            last_ref[k, b : b + 1, LANES : 2 * LANES] = keys[row]
            last_ref[k, b : b + 1, 2 * LANES :] = queries[row]
    last = last_ref[...]
    trail_ref[...] = last[:, :, : 2 * LANES].astype(BF16)
    value_sum = last[0, :, :P_SIZE] * value_taps[:1]
    key_sum = last[0, :, LANES : 2 * LANES] * key_taps[:1]
    query_sum = last[0, :, 2 * LANES :] * query_taps[:1]
    for k in range(1, CONV - 1):
        value_sum = value_sum + last[k, :, :P_SIZE] * value_taps[k : k + 1]
        key_sum = key_sum + last[k, :, LANES : 2 * LANES] * key_taps[k : k + 1]
        query_sum = query_sum + last[k, :, 2 * LANES :] * query_taps[k : k + 1]
    new_input = rounded(silu(value_sum + values[count:] * value_taps[CONV - 1 : CONV]))
    new_in = rounded(silu(key_sum + keys[count:] * key_taps[CONV - 1 : CONV]))
    new_out = rounded(silu(query_sum + queries[count:] * query_taps[CONV - 1 : CONV]))
    step = softplus(new_step + pick(bias_ref[...], head))
    speed = jnp.exp(pick(decay_ref[...], head))
    decay_out_ref[...] = jnp.broadcast_to(jnp.exp(-speed * step), decay_out_ref.shape)
    agreement = jnp.sum(new_in * new_out, axis=1, keepdims=True)
    direct = new_input * (step * agreement + pick(skip_ref[...], head))
    high = rounded(direct)
    direct = jnp.concatenate([high, direct - high], axis=1)
    newest_ref[...] = jnp.concatenate([new_out, direct], axis=0).astype(BF16)
    gate_out_ref[...] = silu(new_gate)


def pack_body(
    halo_ref, lead_ref, weight_ref, logs_ref, taps_ref, state_ref, newest_ref, out_ref,
):
    prompts, rows, _ = state_ref.shape
    padded = logs_ref.shape[0]
    taps = taps_ref[...]
    window = [halo_ref[k].astype(F32) for k in range(CONV - 1)]
    window = window + [lead_ref[k] for k in range(CONV - 1)]
    weighted, maps = [], []
    for t in range(CONV - 1):
        total = window[t] * taps[:1]
        for k in range(1, CONV):
            total = total + window[t + k] * taps[k : k + 1]
        mixed = rounded(silu(total))
        weight = pick(weight_ref[...], t)
        weighted.append(jnp.transpose(rounded(mixed[:, :LANES] * weight)))
        maps.append(mixed[:, LANES:])
    for b in range(prompts):
        state = state_ref[b]
        for t in range(CONV - 1):
            state = state + weighted[t][:rows, b : b + 1] * maps[t][b : b + 1]
        out_ref[b * rows : (b + 1) * rows] = state.astype(BF16)
    base = prompts * rows
    logs = jnp.zeros((padded, LANES), F32)
    for k, part in enumerate(pieces(logs_ref[...])):
        logs = jnp.where(iota(logs.shape, 1) == k, part.astype(F32), logs)
    out_ref[base : base + padded] = logs.astype(BF16)
    out_ref[base + padded :] = newest_ref[...]


def log_of(part_ref, base, padded):
    log = jnp.sum(part_ref[base : base + padded].astype(F32), axis=1, keepdims=True)
    return jnp.broadcast_to(log, (padded, LANES))


def followed(states, part_ref, log):
    decay = jnp.exp(log)
    rows = states[0].shape[0]
    return [
        state * decay[b : b + 1] + part_ref[b * rows : (b + 1) * rows].astype(F32)
        for b, state in enumerate(states)
    ]


def joined_shards(refs, base, padded, prompts):
    rows = base // prompts
    states = [refs[0][b * rows : (b + 1) * rows].astype(F32) for b in range(prompts)]
    for ref in refs[1:]:
        states = followed(states, ref, log_of(ref, base, padded))
    return states


def early_body(*refs, prompts, padded):
    parts, state_ref = refs[:-1], refs[-1]
    states = joined_shards(parts, prompts * P_SIZE, padded, prompts)
    for b in range(prompts):
        state_ref[b] = states[b]


def hub_body(
    state_ref, before_ref, last_ref, decay_ref, gate_ref, own_ref, *next_refs, keep,
):
    prompts, rows, _ = state_ref.shape
    padded = decay_ref.shape[0]
    dests = rows // keep
    base = prompts * rows
    states = [state_ref[b] for b in range(prompts)]
    for ref in (before_ref, last_ref):
        states = followed(states, ref, log_of(ref, base, padded))
    newest = last_ref[base + padded :].astype(F32)
    new_out = newest[:padded]
    lane = iota((rows, LANES), 1)
    reads = jnp.zeros((rows, LANES), F32)
    kept = []
    for b in range(prompts):
        state = rounded(states[b])
        read = jnp.sum(state * new_out[b : b + 1], axis=1, keepdims=True)
        reads = jnp.where(lane == b, read, reads)
        kept.append(state)
    corner = (padded, LANES)
    decay = jnp.where(iota(corner, 0) == iota(corner, 1), decay_ref[...], 0.0)
    decay = jnp.sum(decay, axis=0, keepdims=True)
    below = jnp.zeros((LANES - padded, LANES), F32)
    direct = jnp.transpose(jnp.concatenate([newest[padded:], below], axis=0))
    direct = direct[:rows] + direct[rows:]
    gate = jnp.concatenate([gate_ref[...], gate_ref[...]], axis=1)
    gate = jnp.transpose(jnp.concatenate([gate, below], axis=0))[:rows]
    gated = jnp.where(lane < prompts, (decay * reads + direct) * gate, 0.0)
    squares = jnp.sum(gated * gated, axis=0, keepdims=True)
    count = rows
    square_rows = jnp.zeros(corner, F32)
    for k, part in enumerate(pieces(squares)):
        square_rows = jnp.where(iota(corner, 0) == k, part.astype(F32), square_rows)
    stack = jnp.concatenate([*pieces(gated), square_rows.astype(BF16)], axis=0)
    chosen = (16 * dests, stack.shape[0])
    dest, at, col = iota(chosen, 0) // 16, iota(chosen, 0) % 16, iota(chosen, 1)
    source = jnp.where(
        at < 3 * keep,
        (at // keep) * count + dest * keep + at % keep,
        3 * count + at - 3 * keep,
    )
    extra = dot((col == source).astype(BF16), stack).astype(BF16)

    def place(dest):
        level = dest.bit_length()
        return ((own_ref, *next_refs)[level], dest - (1 << level >> 1))

    pair_rows = 2 * keep
    blocks = count // pair_rows
    first = iota((blocks, pair_rows, STATE), 1) < keep
    for b in range(0, prompts, 2):
        one = kept[b].reshape(blocks, pair_rows, STATE)
        two = kept[b + 1].reshape(blocks, pair_rows, STATE)
        even = jnp.where(first, one, pltpu.roll(two, keep, axis=1)).astype(BF16)
        odd = jnp.where(first, pltpu.roll(one, keep, axis=1), two).astype(BF16)
        for k in range(blocks):
            for dest, value in ((2 * k, even[k]), (2 * k + 1, odd[k])):
                ref, i = place(dest)
                ref[i, b * keep : (b + 2) * keep, :] = value
    for d in range(dests):
        ref, i = place(d)
        ref[i, prompts * keep :, :] = extra[d * 16 : (d + 1) * 16]


def pick_body(own_ref, *refs, places, keep):
    parts, (cache_ref, gated_ref, squares_ref) = refs[:-3], refs[-3:]
    rows = cache_ref.shape[0]
    at_hub = lax.axis_index("sp") == 0
    mine = jnp.where(at_hub, own_ref[0].astype(F32), 0.0)
    for part, place in zip(parts, places):
        mine = mine + part[place].astype(F32)
    mine = mine.astype(BF16)
    cache_ref[...] = mine[:rows]
    shape = (8, 16)
    row, col = iota(shape, 0), iota(shape, 1)
    chosen = ((row < keep) & (col < 3 * keep) & (col % keep == row)) | (
        (row == keep) & (col >= 3 * keep) & (col < 3 * keep + 3)
    )
    values = dot(chosen.astype(BF16), mine[rows:])
    gated_ref[...] = values
    squares_ref[...] = jnp.broadcast_to(values[keep : keep + 1][None], squares_ref.shape)


def final_body(parts_ref, gated_ref, gain_ref, out_ref):
    _, keep, prompts = out_ref.shape
    heads, rows = gain_ref.shape
    head = lax.axis_index(TP)
    shard = lax.axis_index("sp")
    total = jnp.sum(parts_ref[...], axis=0)
    scale = lax.rsqrt(total / (heads * rows) + EPSILON)
    gain = jnp.broadcast_to(pick_row(gain_ref[...], head), (8, rows))
    own = iota((8, rows), 1) == shard * keep + iota((8, rows), 0)
    gain = jnp.sum(jnp.where(own, gain, 0.0), axis=1, keepdims=True)
    out = gated_ref[...] * scale * gain
    out_ref[0] = out[:keep, :prompts].astype(BF16)


def whole(count):
    return [pl.BlockSpec(memory_space=pltpu.VMEM) for _ in range(count)]


def call(body, outs, *operands, specs=None, scratch=()):
    return pl.pallas_call(
        body,
        in_specs=specs or whole(len(operands)),
        out_specs=whole(len(outs)),
        out_shape=outs,
        scratch_shapes=scratch,
    )(*operands)


def shards(
    prompt_layer_input,
    next_token_input,
    value_projection,
    output_gate_matrix,
    key_projection,
    query_projection,
    step_projection,
    value_filter_taps,
    key_filter_taps,
    query_filter_taps,
    step_size_bias,
    head_decay_logarithm,
    direct_path_weight,
    gated_norm_gain,
    position_decay_offset,
):
    prompts, length, width = prompt_layer_input.shape
    dests = lax.axis_size("sp")
    keep = P_SIZE // dests
    padded = -(-prompts // 8) * 8
    bias = step_size_bias[None]
    decay_rate = head_decay_logarithm[None]
    skip = direct_path_weight[None]
    out = jax.ShapeDtypeStruct
    value_rows = value_projection.T
    gate_rows = output_gate_matrix.T
    step_rows = step_projection.T
    offset_rows = jnp.swapaxes(position_decay_offset, 1, 2)

    block = 16
    tail = length // block - 1
    token_operands = (
        key_projection,
        query_projection,
        prompt_layer_input,
        next_token_input,
        value_rows,
        gate_rows,
        step_rows,
        value_filter_taps,
        key_filter_taps,
        query_filter_taps,
        bias,
        decay_rate,
        skip,
    )
    trail, newest, new_decay, new_gate = pl.pallas_call(
        token_body,
        grid=(1,),
        in_specs=[pl.BlockSpec(memory_space=pl.ANY)] * 2
        + [pl.BlockSpec((prompts, block, width), lambda i: (0, tail, 0))]
        + whole(len(token_operands) - 3),
        out_specs=whole(4),
        out_shape=[
            out((CONV - 1, padded, 2 * LANES), BF16),
            out((2 * padded, LANES), BF16),
            out((padded, LANES), F32),
            out((padded, P_SIZE), F32),
        ],
        scratch_shapes=[
            pltpu.VMEM((padded, width), F32),
            pltpu.VMEM((CONV - 1, padded, 3 * LANES), F32),
            pltpu.VMEM((width, STATE), BF16),
            pltpu.VMEM((width, STATE), BF16),
            pltpu.SemaphoreType.DMA((2,)),
        ],
        name="token",
    )(*token_operands)
    halo = lax.ppermute(trail, "sp", [(i, i + 1) for i in range(dests - 1)])
    per = 2
    state, lead, weight, logs, taps = call(
        lambda *refs: local_body(*refs, per=per),
        [
            out((prompts, P_SIZE, STATE), F32),
            out((CONV - 1, padded, 2 * LANES), F32),
            out((padded, length), F32),
            out((padded, LANES), F32),
            out((8, 2 * LANES), F32),
        ],
        prompt_layer_input,
        key_projection,
        value_rows,
        step_rows,
        value_filter_taps,
        key_filter_taps,
        bias,
        decay_rate,
        offset_rows,
        specs=[pl.BlockSpec(memory_space=pl.ANY)] * 2 + whole(7),
        scratch=[
            pltpu.VMEM((prompts, length, width), BF16),
            pltpu.VMEM((width, 2 * LANES), BF16),
            pltpu.VMEM((prompts, P_SIZE, length), F32),
            pltpu.VMEM((prompts, length, STATE), BF16),
            pltpu.VMEM((2, padded, length), F32),
            pltpu.SemaphoreType.DMA,
            pltpu.SemaphoreType.DMA((prompts // per,)),
        ],
    )
    (payload,) = call(
        pack_body,
        [out((prompts * P_SIZE + 3 * padded, STATE), BF16)],
        halo,
        lead,
        weight,
        logs,
        taps,
        state,
        newest,
    )
    parts = [payload]
    for k in range(dests - 1, 0, -1):
        parts.insert(1, lax.ppermute(payload, "sp", [(k, 0)]))
    (early,) = call(
        lambda *refs: early_body(*refs, prompts=prompts, padded=padded),
        [out((prompts, P_SIZE, STATE), F32)],
        *parts[: dests - 2],
    )
    entry = prompts * keep + 16
    own, to1, to2, to4, to8 = call(
        lambda *refs: hub_body(*refs, keep=keep),
        [out((n, entry, STATE), BF16) for n in (1, 1, 2, 4, 8)],
        early,
        parts[dests - 2],
        parts[dests - 1],
        new_decay,
        new_gate,
    )

    def hop(value, *pairs):
        return lax.ppermute(value, "sp", pairs)

    to1 = hop(to1, (0, 1))
    to2 = hop(to2, (0, 2))
    to4 = hop(to4, (0, 4))
    to8 = hop(to8, (0, 8))
    to12 = hop(to8, (8, 12))
    to6 = hop(to4[2:] + to8[2:4] + to12[6:], (4, 6), (8, 10), (12, 14))
    odd = to2[1:] + to4[1:2] + to8[1:2] + to12[5:6] + to6[1:]
    odd = hop(odd, *[(i, i + 1) for i in range(2, dests, 2)])
    places = (0, 0, 0, 0, 4, 0, 0)
    tp_size = lax.axis_size(TP)
    cache, gated, squares = call(
        lambda *refs: pick_body(*refs, places=places, keep=keep),
        [
            out((prompts * keep, STATE), BF16),
            out((8, LANES), F32),
            out((tp_size, 1, LANES), F32),
        ],
        own,
        to1,
        to2,
        to4,
        to8,
        to12,
        to6,
        odd,
    )
    squares = lax.all_to_all(squares, TP, 0, 0, tiled=True)
    (first_read,) = call(
        final_body, [out((1, keep, prompts), BF16)], squares, gated, gated_norm_gain
    )
    return cache.reshape(prompts, 1, keep, STATE), jnp.transpose(first_read, (2, 0, 1))


def solution(mesh):
    split = Mesh(
        mesh.devices.reshape(mesh.shape["grp"], mesh.shape["sp"], mesh.shape["tp"] // 2, 2),
        ("grp", "sp", "tp_0", "tp_1"),
    )
    return jax.shard_map(
        shards,
        mesh=split,
        in_specs=(
            P("grp", "sp", None),
            P("grp", None),
            P(None, TP),
            P(None, TP),
            P(),
            P(),
            P(),
            P(),
            P(),
            P(),
            P(),
            P(),
            P(),
            P(),
            P("grp", "sp", None),
        ),
        out_specs=(P("grp", TP, "sp", None), P("grp", TP, "sp")),
        check_vma=False,
    )
```

```python
import jax
import jax.numpy as jnp
from jax import lax
from jax.experimental import pallas as pl
from jax.experimental.pallas import tpu as pltpu
from jax.sharding import Mesh
from jax.sharding import PartitionSpec as P

HEADS = 32
P_SIZE = 64
GROUPS = 2
STATE = 128
CONV = 4
LANES = 128
TP = ("tp_0", "tp_1")
EPSILON = 1e-06

F32 = jnp.float32
BF16 = jnp.bfloat16


def rounded(value):
    return value.astype(BF16).astype(F32)


def silu(value):
    return value / (1.0 + jnp.exp(-value))


def softplus(value):
    return jnp.maximum(value, 0.0) + jnp.log1p(jnp.exp(-jnp.abs(value)))


def dot(a, b, dims=((1,), (0,))):
    return lax.dot_general(a, b, (dims, ((), ())), preferred_element_type=F32)


def pieces(value):
    first = value.astype(BF16)
    rest = value - first.astype(F32)
    second = rest.astype(BF16)
    third = (rest - second.astype(F32)).astype(BF16)
    return first, second, third


def dot01(matrix, value):
    a, b, c = pieces(value)
    return dot(jnp.concatenate([matrix] * 3, axis=1), jnp.concatenate([a, b, c], axis=0))


def iota(shape, dim):
    return lax.broadcasted_iota(jnp.int32, shape, dim)


def own_half(row, head):
    return jnp.where(head % 2 == 0, row, pltpu.roll(row, 64, axis=1))


def pick(row, lane):
    return jnp.sum(jnp.where(iota(row.shape, 1) == lane, row, 0.0), axis=1, keepdims=True)


def pick_row(matrix, row):
    matrix = matrix.astype(F32)
    return jnp.sum(jnp.where(iota(matrix.shape, 0) == row, matrix, 0.0), axis=0, keepdims=True)


def local_body(
    x_hbm, key_hbm, value_hbm, step_hbm, off_hbm, taps_ref, bias_ref, decay_ref,
    state_ref, lead_ref, weight_ref, logs_ref,
    x_ref, w_ref, value_ref, step_ref, off_ref, wide_ref, map_ref, rows_ref, small_sems, sems,
    *, per,
):
    prompts, length, width = x_hbm.shape
    head = lax.axis_index(TP)
    group = head // (HEADS // GROUPS)
    at = pl.multiple_of(group * STATE, STATE)
    small = (
        (value_hbm, value_ref),
        (step_hbm, step_ref),
        (key_hbm.at[:, pl.ds(at, STATE)], w_ref.at[:, pl.ds(LANES, STATE)]),
        (off_hbm, off_ref),
    )
    small = [pltpu.make_async_copy(*pair, small_sems.at[i]) for i, pair in enumerate(small)]
    for copy in small:
        copy.start()
    copies = []
    for i in range(prompts // per):
        part = pl.ds(i * per, per)
        copies.append(pltpu.make_async_copy(x_hbm.at[part], x_ref.at[part], sems.at[i]))
    for copy in copies:
        copy.start()
    small[0].wait()
    small[1].wait()
    step_row = jnp.broadcast_to(pick_row(step_ref[...], head), (P_SIZE, width)).astype(BF16)
    w_ref[:, :LANES] = jnp.transpose(jnp.concatenate([value_ref[...], step_row], axis=0))
    taps = taps_ref[:CONV]
    rows_ref[...] = jnp.zeros_like(rows_ref)
    small[3].wait()
    offset = off_ref[...]
    offset = jnp.where(iota(offset.shape, 1) == head, offset, 0.0)
    rows_ref[1, :prompts] = jnp.sum(offset, axis=1)
    feature = iota((length, LANES), 1) < P_SIZE
    small[2].wait()
    for i in range(prompts // per):
        copies[i].wait()
        rows = x_ref[i * per : (i + 1) * per].reshape(per * length, width)
        raw_all = rounded(dot(rows, w_ref[...]))
        for j in range(per):
            b = i * per + j
            raw = raw_all[j * length : (j + 1) * length]
            for k in range(CONV - 1):
                lead_ref[k, b : b + 1, :] = raw[k : k + 1]
            total = raw * taps[CONV - 1 : CONV]
            for k in range(CONV - 1):
                total = total + pltpu.roll(raw, CONV - 1 - k, axis=0) * taps[k : k + 1]
            mixed = silu(total)
            map_ref[b] = mixed[:, LANES:].astype(BF16)
            turned = jnp.where(feature, rounded(mixed[:, :LANES]), raw[:, :LANES])
            turned = jnp.transpose(turned)
            wide_ref[b] = turned[:P_SIZE]
            rows_ref[0, b : b + 1, :] = turned[P_SIZE : P_SIZE + 1]
    step = softplus(rows_ref[0] + pick(bias_ref[...], head))
    log = rows_ref[1] - jnp.exp(pick(decay_ref[...], head)) * step
    later = (iota((length, length), 0) > iota((length, length), 1)).astype(BF16)
    after = dot(jnp.concatenate(pieces(log), axis=1), jnp.concatenate([later] * 3, axis=0))
    weight = jnp.exp(after) * step
    weight_ref[...] = weight
    logs_ref[...] = jnp.broadcast_to(jnp.sum(log, axis=1, keepdims=True), logs_ref.shape)
    weight = jnp.where(iota(weight.shape, 1) >= CONV - 1, weight, 0.0)
    for b in range(prompts):
        weighted = (wide_ref[b] * weight[b : b + 1]).astype(BF16)
        state_ref[b] = dot(weighted, map_ref[b])


def taps_of(vt_ref, kt_ref):
    head = lax.axis_index(TP)
    at = pl.multiple_of((head // (HEADS // GROUPS)) * STATE, STATE)
    pair = pl.multiple_of((head // 2) * LANES, LANES)
    value_taps = own_half(vt_ref[:, pl.ds(pair, LANES)].astype(F32), head)
    return jnp.concatenate([value_taps, kt_ref[:, pl.ds(at, STATE)].astype(F32)], axis=1)


def on_last():
    return lax.axis_index("sp") == lax.axis_size("sp") - 1


def early_body(
    x_hbm, key_hbm, value_hbm, step_hbm, off_hbm, vt_ref, kt_ref, bias_ref, decay_ref,
    state_ref, lead_ref, weight_ref, logs_ref, taps_ref, *scratch, per,
):
    taps_ref[:CONV] = taps_of(vt_ref, kt_ref)

    @pl.when(jnp.logical_not(on_last()))
    def _():
        local_body(
            x_hbm, key_hbm, value_hbm, step_hbm, off_hbm, taps_ref, bias_ref, decay_ref,
            state_ref, lead_ref, weight_ref, logs_ref, *scratch, per=per,
        )


def late_body(
    x_hbm, key_hbm, value_hbm, step_hbm, off_hbm, taps_ref, bias_ref, decay_ref, after_ref,
    state_in, lead_in, weight_in, logs_in,
    state_ref, lead_ref, weight_ref, logs_ref, *scratch, per,
):
    @pl.when(on_last())
    def _():
        local_body(
            x_hbm, key_hbm, value_hbm, step_hbm, off_hbm, taps_ref, bias_ref, decay_ref,
            state_ref, lead_ref, weight_ref, logs_ref, *scratch, per=per,
        )

    @pl.when(jnp.logical_not(on_last()))
    def _():
        copies = []
        inputs = (state_in, lead_in, weight_in, logs_in)
        outputs = (state_ref, lead_ref, weight_ref, logs_ref)
        for i, (source, target) in enumerate(zip(inputs, outputs)):
            copies.append(pltpu.make_async_copy(source, target, scratch[-2].at[i]))
        for copy in copies:
            copy.start()
        for copy in copies:
            copy.wait()


def token_body(
    x_ref, next_ref, value_ref, gate_ref, key_ref, query_ref, step_ref, taps_ref, qt_ref,
    bias_ref, decay_ref, skip_ref,
    trail_ref, newest_ref, decay_out_ref, gate_out_ref,
    pad_ref, last_ref,
):
    prompts, block, width = x_ref.shape
    head = lax.axis_index(TP)
    group = head // (HEADS // GROUPS)
    padded = pad_ref.shape[0]
    at = pl.multiple_of(group * STATE, STATE)
    query = query_ref[:, pl.ds(at, STATE)]
    key = key_ref[:, pl.ds(at, STATE)]
    value_taps = taps_ref[:CONV, :P_SIZE]
    key_taps = taps_ref[:CONV, LANES:]
    query_taps = qt_ref[:, pl.ds(at, STATE)].astype(F32)
    pad_ref[...] = jnp.zeros_like(pad_ref)
    pad_ref[:prompts] = next_ref[...].astype(F32)
    token = pad_ref[...].astype(BF16)
    rows = jnp.concatenate([x_ref[...].reshape(prompts * block, width), token], axis=0)
    count = prompts * block
    values = rounded(dot(rows, value_ref[...], ((1,), (1,))))
    keys = rounded(dot(rows, key))
    queries = rounded(dot(rows, query))
    new_step = pick(rounded(dot(token, step_ref[...], ((1,), (1,)))), head)
    new_gate = rounded(dot(token, gate_ref[...], ((1,), (1,))))
    last_ref[...] = jnp.zeros_like(last_ref)
    for b in range(prompts):
        at_row = (b + 1) * block - (CONV - 1)
        for k in range(CONV - 1):
            row = slice(at_row + k, at_row + k + 1)
            last_ref[k, b : b + 1, :P_SIZE] = values[row]
            last_ref[k, b : b + 1, LANES : 2 * LANES] = keys[row]
            last_ref[k, b : b + 1, 2 * LANES :] = queries[row]
    last = last_ref[...]
    trail_ref[...] = last[:, :, : 2 * LANES].astype(BF16)
    value_sum = last[0, :, :P_SIZE] * value_taps[:1]
    key_sum = last[0, :, LANES : 2 * LANES] * key_taps[:1]
    query_sum = last[0, :, 2 * LANES :] * query_taps[:1]
    for k in range(1, CONV - 1):
        value_sum = value_sum + last[k, :, :P_SIZE] * value_taps[k : k + 1]
        key_sum = key_sum + last[k, :, LANES : 2 * LANES] * key_taps[k : k + 1]
        query_sum = query_sum + last[k, :, 2 * LANES :] * query_taps[k : k + 1]
    new_input = rounded(silu(value_sum + values[count:] * value_taps[CONV - 1 : CONV]))
    new_in = rounded(silu(key_sum + keys[count:] * key_taps[CONV - 1 : CONV]))
    new_out = rounded(silu(query_sum + queries[count:] * query_taps[CONV - 1 : CONV]))
    step = softplus(new_step + pick(bias_ref[...], head))
    speed = jnp.exp(pick(decay_ref[...], head))
    decay_out_ref[...] = jnp.broadcast_to(jnp.exp(-speed * step), decay_out_ref.shape)
    agreement = jnp.sum(new_in * new_out, axis=1, keepdims=True)
    direct = new_input * (step * agreement + pick(skip_ref[...], head))
    high = rounded(direct)
    direct = jnp.concatenate([high, direct - high], axis=1)
    newest = jnp.concatenate([new_out, direct], axis=0).astype(BF16)
    for d in range(newest_ref.shape[0]):
        newest_ref[d] = newest
    gate_out_ref[...] = silu(new_gate)


def pack_body(
    halo_ref, lead_ref, weight_ref, logs_ref, taps_ref, state_ref, newest_ref, out_ref,
):
    prompts, rows, _ = state_ref.shape
    dests = out_ref.shape[0]
    keep = rows // dests
    padded = logs_ref.shape[0]
    taps = taps_ref[...]
    new_out = newest_ref[dests - 1, :padded, :].astype(F32)
    window = [halo_ref[k].astype(F32) for k in range(CONV - 1)]
    window = window + [lead_ref[k] for k in range(CONV - 1)]
    weighted, maps = [], []
    for t in range(CONV - 1):
        total = window[t] * taps[:1]
        for k in range(1, CONV):
            total = total + window[t + k] * taps[k : k + 1]
        mixed = rounded(silu(total))
        weight = pick(weight_ref[...], t)
        weighted.append(jnp.transpose(rounded(mixed[:, :LANES] * weight)))
        maps.append(mixed[:, LANES:])
    states = []
    reads = jnp.zeros((rows, LANES), F32)
    lane = iota((rows, LANES), 1)
    for b in range(prompts):
        state = state_ref[b]
        for t in range(CONV - 1):
            state = state + weighted[t][:rows, b : b + 1] * maps[t][b : b + 1]
        states.append(state)
        read = jnp.sum(state * new_out[b : b + 1], axis=1, keepdims=True)
        reads = jnp.where(lane == b, read, reads)
    pair_rows = 2 * keep
    blocks = rows // pair_rows
    low = iota((blocks, pair_rows, STATE), 1) < keep
    for b in range(0, prompts, 2):
        one = states[b].reshape(blocks, pair_rows, STATE)
        two = states[b + 1].reshape(blocks, pair_rows, STATE)
        even = jnp.where(low, one, pltpu.roll(two, keep, axis=1))
        odd = jnp.where(low, pltpu.roll(one, keep, axis=1), two)
        at = b * keep
        for k in range(blocks):
            out_ref[2 * k, at : at + pair_rows, :] = even[k].astype(BF16)
            out_ref[2 * k + 1, at : at + pair_rows, :] = odd[k].astype(BF16)
    reads = jnp.transpose(reads)[:padded]
    high = rounded(reads)
    extra = jnp.concatenate([high, reads - high], axis=1)
    corner = (padded, LANES)
    logs = jnp.where(iota(corner, 0) == iota(corner, 1), logs_ref[...], 0.0)
    logs = jnp.sum(logs, axis=0, keepdims=True)
    for k, part in enumerate(pieces(logs)):
        extra = jnp.where(iota(corner, 0) == prompts + k, part.astype(F32), extra)
    extra = extra.astype(BF16)
    for d in range(dests):
        out_ref[d, prompts * keep :, :] = extra


def read_body(
    parts_ref, newest_ref, decay_ref, gate_ref, cache_ref, gated_ref, squares_ref, *, prompts,
):
    sources, _, _ = parts_ref.shape
    padded = decay_ref.shape[0]
    rows = parts_ref.shape[1] - padded
    keep = rows // prompts
    shard = lax.axis_index("sp")
    state_own = iota((rows, LANES), 1) == iota((rows, LANES), 0) // keep
    read_own = iota((padded, LANES), 1) == iota((padded, LANES), 0)
    total = jnp.zeros((rows, STATE), F32)
    reads = jnp.zeros((padded, P_SIZE), F32)
    for s in range(sources):
        extra = parts_ref[s, rows:, :].astype(F32)
        decay = jnp.sum(extra[prompts : prompts + 3], axis=0, keepdims=True)
        decay = jnp.exp(decay)
        per_row = jnp.sum(jnp.where(state_own, decay, 0.0), axis=1, keepdims=True)
        per_prompt = jnp.sum(jnp.where(read_own, decay, 0.0), axis=1, keepdims=True)
        total = total * per_row + parts_ref[s, :rows, :].astype(F32)
        reads = reads * per_prompt + (extra[:, :P_SIZE] + extra[:, P_SIZE:])
    cache_ref[...] = total.astype(BF16)
    direct = newest_ref[sources - 1, padded:, :].astype(F32)
    direct = direct[:, :P_SIZE] + direct[:, P_SIZE:]
    gated = (decay_ref[:, :P_SIZE] * reads + direct) * gate_ref[...]
    gated = jnp.where(iota(gated.shape, 0) < prompts, gated, 0.0)
    squares = jnp.sum(gated * gated, axis=1, keepdims=True)
    squares = jnp.sum(jnp.where(read_own, squares, 0.0), axis=0, keepdims=True)
    squares_ref[...] = jnp.broadcast_to(squares[None], squares_ref.shape)
    square = jnp.concatenate([gated, jnp.zeros((P_SIZE - padded, P_SIZE), F32)], axis=0)
    square = jnp.concatenate([square, jnp.zeros((P_SIZE, P_SIZE), F32)], axis=0)
    square = jnp.concatenate([square, jnp.zeros((LANES, P_SIZE), F32)], axis=1)
    own = (iota((8, LANES), 1) == shard * keep + iota((8, LANES), 0)).astype(BF16)
    gated_ref[...] = dot01(own, jnp.transpose(square))


def final_body(parts_ref, gated_ref, gain_ref, out_ref):
    _, keep, prompts = out_ref.shape
    heads, rows = gain_ref.shape
    head = lax.axis_index(TP)
    shard = lax.axis_index("sp")
    total = jnp.sum(parts_ref[...], axis=0)
    scale = lax.rsqrt(total / (heads * rows) + EPSILON)
    gain = jnp.broadcast_to(pick_row(gain_ref[...], head), (8, rows))
    own = iota((8, rows), 1) == shard * keep + iota((8, rows), 0)
    gain = jnp.sum(jnp.where(own, gain, 0.0), axis=1, keepdims=True)
    out = gated_ref[...] * scale * gain
    out_ref[0] = out[:keep, :prompts].astype(BF16)


def whole(count):
    return [pl.BlockSpec(memory_space=pltpu.VMEM) for _ in range(count)]


def call(body, outs, *operands, specs=None, scratch=(), name=None):
    return pl.pallas_call(
        body,
        in_specs=specs or whole(len(operands)),
        out_specs=whole(len(outs)),
        out_shape=outs,
        scratch_shapes=scratch,
        name=name,
    )(*operands)


def shards(
    prompt_layer_input,
    next_token_input,
    value_projection,
    output_gate_matrix,
    key_projection,
    query_projection,
    step_projection,
    value_filter_taps,
    key_filter_taps,
    query_filter_taps,
    step_size_bias,
    head_decay_logarithm,
    direct_path_weight,
    gated_norm_gain,
    position_decay_offset,
):
    prompts, length, width = prompt_layer_input.shape
    dests = lax.axis_size("sp")
    keep = P_SIZE // dests
    padded = -(-prompts // 8) * 8
    bias = step_size_bias[None]
    decay_rate = head_decay_logarithm[None]
    skip = direct_path_weight[None]
    out = jax.ShapeDtypeStruct
    value_rows = value_projection.T
    gate_rows = output_gate_matrix.T
    step_rows = step_projection.T
    offset_rows = jnp.swapaxes(position_decay_offset, 1, 2)

    per = 2
    local_outs = [
        out((prompts, P_SIZE, STATE), F32),
        out((CONV - 1, padded, 2 * LANES), F32),
        out((padded, length), F32),
        out((padded, LANES), F32),
    ]
    local_operands = (
        prompt_layer_input,
        key_projection,
        value_rows,
        step_rows,
        offset_rows,
    )
    away = [pl.BlockSpec(memory_space=pl.ANY)]
    local_scratch = [
        pltpu.VMEM((prompts, length, width), BF16),
        pltpu.VMEM((width, 2 * LANES), BF16),
        pltpu.VMEM(value_rows.shape, BF16),
        pltpu.VMEM(step_rows.shape, BF16),
        pltpu.VMEM(offset_rows.shape, F32),
        pltpu.VMEM((prompts, P_SIZE, length), F32),
        pltpu.VMEM((prompts, length, STATE), BF16),
        pltpu.VMEM((2, padded, length), F32),
        pltpu.SemaphoreType.DMA((4,)),
        pltpu.SemaphoreType.DMA((prompts // per,)),
    ]
    *early, taps = call(
        lambda *refs: early_body(*refs, per=per),
        [*local_outs, out((8, 2 * LANES), F32)],
        *local_operands,
        value_filter_taps,
        key_filter_taps,
        bias,
        decay_rate,
        specs=away * 5 + whole(4),
        scratch=local_scratch,
        name="early",
    )
    block = 16
    tail = length // block - 1
    token_operands = (
        prompt_layer_input,
        next_token_input,
        value_rows,
        gate_rows,
        key_projection,
        query_projection,
        step_rows,
        taps,
        query_filter_taps,
        bias,
        decay_rate,
        skip,
    )
    trail, newest, new_decay, new_gate = pl.pallas_call(
        token_body,
        grid=(1,),
        in_specs=[pl.BlockSpec((prompts, block, width), lambda i: (0, tail, 0))]
        + whole(len(token_operands) - 1),
        out_specs=whole(4),
        out_shape=[
            out((CONV - 1, padded, 2 * LANES), BF16),
            out((dests, 2 * padded, LANES), BF16),
            out((padded, LANES), F32),
            out((padded, P_SIZE), F32),
        ],
        scratch_shapes=[
            pltpu.VMEM((padded, width), F32),
            pltpu.VMEM((CONV - 1, padded, 3 * LANES), F32),
        ],
        name="token",
    )(*token_operands)
    newest = lax.all_to_all(newest, "sp", 0, 0, tiled=True)
    halo = lax.ppermute(trail, "sp", [(i, i + 1) for i in range(dests - 1)])
    state, lead, weight, logs = call(
        lambda *refs: late_body(*refs, per=per),
        local_outs,
        *local_operands,
        taps,
        bias,
        decay_rate,
        new_decay,
        *early,
        specs=away * 5 + whole(3) + away * 5,
        scratch=local_scratch,
        name="late",
    )
    (payload,) = call(
        pack_body,
        [out((dests, prompts * keep + padded, STATE), BF16)],
        halo,
        lead,
        weight,
        logs,
        taps,
        state,
        newest,
        name="pack",
    )
    received = lax.all_to_all(payload, "sp", 0, 0, tiled=True)
    tp_size = lax.axis_size(TP)
    cache, gated, squares = call(
        lambda *refs: read_body(*refs, prompts=prompts),
        [
            out((prompts * keep, STATE), BF16),
            out((8, LANES), F32),
            out((tp_size, 1, LANES), F32),
        ],
        received,
        newest,
        new_decay,
        new_gate,
        name="read",
    )
    squares = lax.all_to_all(squares, TP, 0, 0, tiled=True)
    (first_read,) = call(
        final_body, [out((1, keep, prompts), BF16)], squares, gated, gated_norm_gain, name="final"
    )
    return cache.reshape(prompts, 1, keep, STATE), jnp.transpose(first_read, (2, 0, 1))


def solution(mesh):
    split = Mesh(
        mesh.devices.reshape(mesh.shape["grp"], mesh.shape["sp"], mesh.shape["tp"] // 2, 2),
        ("grp", "sp", "tp_0", "tp_1"),
    )
    return jax.shard_map(
        shards,
        mesh=split,
        in_specs=(
            P("grp", "sp", None),
            P("grp", None),
            P(None, TP),
            P(None, TP),
            P(),
            P(),
            P(),
            P(),
            P(),
            P(),
            P(),
            P(),
            P(),
            P(),
            P("grp", "sp", None),
        ),
        out_specs=(P("grp", TP, "sp", None), P("grp", TP, "sp")),
        check_vma=False,
    )
```

```python
import jax
import jax.numpy as jnp
from jax import lax
from jax.experimental import pallas as pl
from jax.experimental.pallas import tpu as pltpu
from jax.sharding import Mesh
from jax.sharding import PartitionSpec as P

HEADS = 32
P_SIZE = 64
GROUPS = 2
STATE = 128
CONV = 4
LANES = 128
TP = ("tp_0", "tp_1")
EPSILON = 1e-06

F32 = jnp.float32
BF16 = jnp.bfloat16


def rounded(value):
    return value.astype(BF16).astype(F32)


def silu(value):
    return value / (1.0 + jnp.exp(-value))


def softplus(value):
    return jnp.maximum(value, 0.0) + jnp.log1p(jnp.exp(-jnp.abs(value)))


def dot(a, b, dims=((1,), (0,))):
    return lax.dot_general(a, b, (dims, ((), ())), preferred_element_type=F32)


def pieces(value):
    first = value.astype(BF16)
    rest = value - first.astype(F32)
    second = rest.astype(BF16)
    third = (rest - second.astype(F32)).astype(BF16)
    return first, second, third


def dot01(matrix, value):
    a, b, c = pieces(value)
    return dot(jnp.concatenate([matrix] * 3, axis=1), jnp.concatenate([a, b, c], axis=0))


def iota(shape, dim):
    return lax.broadcasted_iota(jnp.int32, shape, dim)


def own_half(row, head):
    return jnp.where(head % 2 == 0, row, pltpu.roll(row, 64, axis=1))


def pick(row, lane):
    return jnp.sum(jnp.where(iota(row.shape, 1) == lane, row, 0.0), axis=1, keepdims=True)


def pick_row(matrix, row):
    matrix = matrix.astype(F32)
    return jnp.sum(jnp.where(iota(matrix.shape, 0) == row, matrix, 0.0), axis=0, keepdims=True)


def local_body(
    x_hbm, key_hbm, value_hbm, step_hbm, off_hbm, taps_ref, bias_ref, decay_ref,
    state_hbm, lead_hbm, weight_hbm, logs_hbm,
    x_ref, w_ref, value_ref, step_ref, off_ref, wide_ref, map_ref, rows_ref,
    state_ref, lead_ref, weight_ref, logs_ref, small_sems, sems,
    *, per,
):
    prompts, length, width = x_hbm.shape
    head = lax.axis_index(TP)
    group = head // (HEADS // GROUPS)
    at = pl.multiple_of(group * STATE, STATE)
    small = (
        (value_hbm, value_ref),
        (step_hbm, step_ref),
        (key_hbm.at[:, pl.ds(at, STATE)], w_ref.at[:, pl.ds(LANES, STATE)]),
        (off_hbm, off_ref),
    )
    small = [pltpu.make_async_copy(*pair, small_sems.at[i]) for i, pair in enumerate(small)]
    for copy in small:
        copy.start()
    copies = []
    for i in range(prompts // per):
        part = pl.ds(i * per, per)
        copies.append(pltpu.make_async_copy(x_hbm.at[part], x_ref.at[part], sems.at[i]))
    for copy in copies:
        copy.start()
    small[0].wait()
    small[1].wait()
    step_row = jnp.broadcast_to(pick_row(step_ref[...], head), (P_SIZE, width)).astype(BF16)
    w_ref[:, :LANES] = jnp.transpose(jnp.concatenate([value_ref[...], step_row], axis=0))
    taps = taps_ref[:CONV]
    rows_ref[...] = jnp.zeros_like(rows_ref)
    small[3].wait()
    offset = off_ref[...]
    offset = jnp.where(iota(offset.shape, 1) == head, offset, 0.0)
    rows_ref[1, :prompts] = jnp.sum(offset, axis=1)
    feature = iota((length, LANES), 1) < P_SIZE
    small[2].wait()
    for i in range(prompts // per):
        copies[i].wait()
        rows = x_ref[i * per : (i + 1) * per].reshape(per * length, width)
        raw_all = rounded(dot(rows, w_ref[...]))
        for j in range(per):
            b = i * per + j
            raw = raw_all[j * length : (j + 1) * length]
            for k in range(CONV - 1):
                lead_ref[k, b : b + 1, :] = raw[k : k + 1]
            total = raw * taps[CONV - 1 : CONV]
            for k in range(CONV - 1):
                total = total + pltpu.roll(raw, CONV - 1 - k, axis=0) * taps[k : k + 1]
            mixed = silu(total)
            map_ref[b] = mixed[:, LANES:].astype(BF16)
            turned = jnp.where(feature, rounded(mixed[:, :LANES]), raw[:, :LANES])
            turned = jnp.transpose(turned)
            wide_ref[b] = turned[:P_SIZE]
            rows_ref[0, b : b + 1, :] = turned[P_SIZE : P_SIZE + 1]
    step = softplus(rows_ref[0] + pick(bias_ref[...], head))
    log = rows_ref[1] - jnp.exp(pick(decay_ref[...], head)) * step
    later = (iota((length, length), 0) > iota((length, length), 1)).astype(BF16)
    after = dot(jnp.concatenate(pieces(log), axis=1), jnp.concatenate([later] * 3, axis=0))
    weight = jnp.exp(after) * step
    weight_ref[...] = weight
    logs_ref[...] = jnp.broadcast_to(jnp.sum(log, axis=1, keepdims=True), logs_ref.shape)
    weight = jnp.where(iota(weight.shape, 1) >= CONV - 1, weight, 0.0)
    for b in range(prompts):
        weighted = (wide_ref[b] * weight[b : b + 1]).astype(BF16)
        state_ref[b] = dot(weighted, map_ref[b])
    results = (
        (state_ref, state_hbm),
        (lead_ref, lead_hbm),
        (weight_ref, weight_hbm),
        (logs_ref, logs_hbm),
    )
    results = [pltpu.make_async_copy(*pair, small_sems.at[i]) for i, pair in enumerate(results)]
    for copy in results:
        copy.start()
    for copy in results:
        copy.wait()


def taps_of(vt_ref, kt_ref):
    head = lax.axis_index(TP)
    at = pl.multiple_of((head // (HEADS // GROUPS)) * STATE, STATE)
    pair = pl.multiple_of((head // 2) * LANES, LANES)
    value_taps = own_half(vt_ref[:, pl.ds(pair, LANES)].astype(F32), head)
    return jnp.concatenate([value_taps, kt_ref[:, pl.ds(at, STATE)].astype(F32)], axis=1)


def is_late():
    return lax.axis_index("sp") >= lax.axis_size("sp") - 2


def early_body(
    x_hbm, key_hbm, value_hbm, step_hbm, off_hbm, vt_ref, kt_ref, bias_ref, decay_ref,
    state_ref, lead_ref, weight_ref, logs_ref, taps_ref, *scratch, per,
):
    taps_ref[:CONV] = taps_of(vt_ref, kt_ref)

    @pl.when(jnp.logical_not(is_late()))
    def _():
        local_body(
            x_hbm, key_hbm, value_hbm, step_hbm, off_hbm, taps_ref, bias_ref, decay_ref,
            state_ref, lead_ref, weight_ref, logs_ref, *scratch, per=per,
        )


def late_body(
    x_hbm, key_hbm, value_hbm, step_hbm, off_hbm, taps_ref, bias_ref, decay_ref, after_ref,
    state_in, lead_in, weight_in, logs_in,
    state_ref, lead_ref, weight_ref, logs_ref, *scratch, per,
):
    @pl.when(is_late())
    def _():
        local_body(
            x_hbm, key_hbm, value_hbm, step_hbm, off_hbm, taps_ref, bias_ref, decay_ref,
            state_ref, lead_ref, weight_ref, logs_ref, *scratch, per=per,
        )


def token_body(
    x_hbm, value_hbm, gate_hbm, step_hbm, key_hbm, query_hbm, next_ref, taps_ref, qt_ref,
    bias_ref, decay_ref, skip_ref,
    trail_ref, newest_ref, decay_out_ref, gate_out_ref,
    x_ref, rows_ref, maps_ref, pad_ref, last_ref, sems,
):
    prompts, block, width = x_ref.shape
    head = lax.axis_index(TP)
    padded = pad_ref.shape[0]
    heads = step_hbm.shape[0]
    at = pl.multiple_of((head // (HEADS // GROUPS)) * STATE, STATE)
    tail = x_hbm.shape[1] - block
    copies = (
        (key_hbm.at[:, pl.ds(at, STATE)], maps_ref.at[:, pl.ds(0, STATE)]),
        (query_hbm.at[:, pl.ds(at, STATE)], maps_ref.at[:, pl.ds(STATE, STATE)]),
        (value_hbm, rows_ref.at[pl.ds(0, P_SIZE)]),
        (gate_hbm, rows_ref.at[pl.ds(P_SIZE, P_SIZE)]),
        (step_hbm, rows_ref.at[pl.ds(2 * P_SIZE, heads)]),
        (x_hbm.at[:, pl.ds(tail, block)], x_ref),
    )
    copies = [pltpu.make_async_copy(*pair, sems.at[i]) for i, pair in enumerate(copies)]
    for copy in copies:
        copy.start()
    value_taps = taps_ref[:CONV, :P_SIZE]
    key_taps = taps_ref[:CONV, LANES:]
    query_taps = qt_ref[:, pl.ds(at, STATE)].astype(F32)
    pad_ref[...] = jnp.zeros_like(pad_ref)
    pad_ref[:prompts] = next_ref[...].astype(F32)
    token = pad_ref[...].astype(BF16)
    for copy in copies:
        copy.wait()
    rows = jnp.concatenate([x_ref[...].reshape(prompts * block, width), token], axis=0)
    count = prompts * block
    maps = rounded(dot(rows, maps_ref[...]))
    keys, queries = maps[:, :STATE], maps[:, STATE:]
    others = rounded(dot(rows, rows_ref[...], ((1,), (1,))))
    values = others[:, :P_SIZE]
    new_gate = others[count:, P_SIZE : 2 * P_SIZE]
    new_step = pick(others[count:, 2 * P_SIZE :], head)
    last_ref[...] = jnp.zeros_like(last_ref)
    for b in range(prompts):
        at_row = (b + 1) * block - (CONV - 1)
        for k in range(CONV - 1):
            row = slice(at_row + k, at_row + k + 1)
            last_ref[k, b : b + 1, :P_SIZE] = values[row]
            last_ref[k, b : b + 1, LANES : 2 * LANES] = keys[row]
            last_ref[k, b : b + 1, 2 * LANES :] = queries[row]
    last = last_ref[...]
    trail_ref[...] = last[:, :, : 2 * LANES].astype(BF16)
    value_sum = last[0, :, :P_SIZE] * value_taps[:1]
    key_sum = last[0, :, LANES : 2 * LANES] * key_taps[:1]
    query_sum = last[0, :, 2 * LANES :] * query_taps[:1]
    for k in range(1, CONV - 1):
        value_sum = value_sum + last[k, :, :P_SIZE] * value_taps[k : k + 1]
        key_sum = key_sum + last[k, :, LANES : 2 * LANES] * key_taps[k : k + 1]
        query_sum = query_sum + last[k, :, 2 * LANES :] * query_taps[k : k + 1]
    new_input = rounded(silu(value_sum + values[count:] * value_taps[CONV - 1 : CONV]))
    new_in = rounded(silu(key_sum + keys[count:] * key_taps[CONV - 1 : CONV]))
    new_out = rounded(silu(query_sum + queries[count:] * query_taps[CONV - 1 : CONV]))
    step = softplus(new_step + pick(bias_ref[...], head))
    speed = jnp.exp(pick(decay_ref[...], head))
    decay_out_ref[...] = jnp.broadcast_to(jnp.exp(-speed * step), decay_out_ref.shape)
    agreement = jnp.sum(new_in * new_out, axis=1, keepdims=True)
    direct = new_input * (step * agreement + pick(skip_ref[...], head))
    high = rounded(direct)
    direct = jnp.concatenate([high, direct - high], axis=1)
    newest = jnp.concatenate([new_out, direct], axis=0).astype(BF16)
    for d in range(newest_ref.shape[0]):
        newest_ref[d] = newest
    gate_out_ref[...] = silu(new_gate)


def pack_body(
    halo_ref, lead_ref, weight_ref, logs_ref, taps_ref, state_ref, newest_ref, out_ref,
):
    prompts, rows, _ = state_ref.shape
    dests = out_ref.shape[0]
    keep = rows // dests
    padded = logs_ref.shape[0]
    taps = taps_ref[...]
    new_out = newest_ref[dests - 1, :padded, :].astype(F32)
    window = [halo_ref[k].astype(F32) for k in range(CONV - 1)]
    window = window + [lead_ref[k] for k in range(CONV - 1)]
    weighted, maps = [], []
    for t in range(CONV - 1):
        total = window[t] * taps[:1]
        for k in range(1, CONV):
            total = total + window[t + k] * taps[k : k + 1]
        mixed = rounded(silu(total))
        weight = pick(weight_ref[...], t)
        weighted.append(jnp.transpose(rounded(mixed[:, :LANES] * weight)))
        maps.append(mixed[:, LANES:])
    states = []
    reads = jnp.zeros((rows, LANES), F32)
    lane = iota((rows, LANES), 1)
    for b in range(prompts):
        state = state_ref[b]
        for t in range(CONV - 1):
            state = state + weighted[t][:rows, b : b + 1] * maps[t][b : b + 1]
        states.append(state)
        read = jnp.sum(state * new_out[b : b + 1], axis=1, keepdims=True)
        reads = jnp.where(lane == b, read, reads)
    pair_rows = 2 * keep
    blocks = rows // pair_rows
    low = iota((blocks, pair_rows, STATE), 1) < keep
    for b in range(0, prompts, 2):
        one = states[b].reshape(blocks, pair_rows, STATE)
        two = states[b + 1].reshape(blocks, pair_rows, STATE)
        even = jnp.where(low, one, pltpu.roll(two, keep, axis=1))
        odd = jnp.where(low, pltpu.roll(one, keep, axis=1), two)
        at = b * keep
        for k in range(blocks):
            out_ref[2 * k, at : at + pair_rows, :] = even[k].astype(BF16)
            out_ref[2 * k + 1, at : at + pair_rows, :] = odd[k].astype(BF16)
    reads = jnp.transpose(reads)[:padded]
    high = rounded(reads)
    extra = jnp.concatenate([high, reads - high], axis=1)
    corner = (padded, LANES)
    logs = jnp.where(iota(corner, 0) == iota(corner, 1), logs_ref[...], 0.0)
    logs = jnp.sum(logs, axis=0, keepdims=True)
    for k, part in enumerate(pieces(logs)):
        extra = jnp.where(iota(corner, 0) == prompts + k, part.astype(F32), extra)
    extra = extra.astype(BF16)
    for d in range(dests):
        out_ref[d, prompts * keep :, :] = extra


def read_body(
    parts_ref, newest_ref, decay_ref, gate_ref, cache_ref, gated_ref, squares_ref, *, prompts,
):
    sources, _, _ = parts_ref.shape
    padded = decay_ref.shape[0]
    rows = parts_ref.shape[1] - padded
    keep = rows // prompts
    shard = lax.axis_index("sp")
    state_own = iota((rows, LANES), 1) == iota((rows, LANES), 0) // keep
    read_own = iota((padded, LANES), 1) == iota((padded, LANES), 0)
    total = jnp.zeros((rows, STATE), F32)
    reads = jnp.zeros((padded, P_SIZE), F32)
    for s in range(sources):
        extra = parts_ref[s, rows:, :].astype(F32)
        decay = jnp.sum(extra[prompts : prompts + 3], axis=0, keepdims=True)
        decay = jnp.exp(decay)
        per_row = jnp.sum(jnp.where(state_own, decay, 0.0), axis=1, keepdims=True)
        per_prompt = jnp.sum(jnp.where(read_own, decay, 0.0), axis=1, keepdims=True)
        total = total * per_row + parts_ref[s, :rows, :].astype(F32)
        reads = reads * per_prompt + (extra[:, :P_SIZE] + extra[:, P_SIZE:])
    cache_ref[...] = total.astype(BF16)
    direct = newest_ref[sources - 1, padded:, :].astype(F32)
    direct = direct[:, :P_SIZE] + direct[:, P_SIZE:]
    gated = (decay_ref[:, :P_SIZE] * reads + direct) * gate_ref[...]
    gated = jnp.where(iota(gated.shape, 0) < prompts, gated, 0.0)
    squares = jnp.sum(gated * gated, axis=1, keepdims=True)
    squares = jnp.sum(jnp.where(read_own, squares, 0.0), axis=0, keepdims=True)
    squares_ref[...] = jnp.broadcast_to(squares[None], squares_ref.shape)
    square = jnp.concatenate([gated, jnp.zeros((P_SIZE - padded, P_SIZE), F32)], axis=0)
    square = jnp.concatenate([square, jnp.zeros((P_SIZE, P_SIZE), F32)], axis=0)
    square = jnp.concatenate([square, jnp.zeros((LANES, P_SIZE), F32)], axis=1)
    own = (iota((8, LANES), 1) == shard * keep + iota((8, LANES), 0)).astype(BF16)
    gated_ref[...] = dot01(own, jnp.transpose(square))


def final_body(parts_ref, gated_ref, gain_ref, out_ref):
    _, keep, prompts = out_ref.shape
    heads, rows = gain_ref.shape
    head = lax.axis_index(TP)
    shard = lax.axis_index("sp")
    total = jnp.sum(parts_ref[...], axis=0)
    scale = lax.rsqrt(total / (heads * rows) + EPSILON)
    gain = jnp.broadcast_to(pick_row(gain_ref[...], head), (8, rows))
    own = iota((8, rows), 1) == shard * keep + iota((8, rows), 0)
    gain = jnp.sum(jnp.where(own, gain, 0.0), axis=1, keepdims=True)
    out = gated_ref[...] * scale * gain
    out_ref[0] = out[:keep, :prompts].astype(BF16)


def whole(count):
    return [pl.BlockSpec(memory_space=pltpu.VMEM) for _ in range(count)]


def call(body, outs, *operands, specs=None, out_specs=None, scratch=(), aliases=(), name=None):
    return pl.pallas_call(
        body,
        in_specs=specs or whole(len(operands)),
        out_specs=out_specs or whole(len(outs)),
        input_output_aliases=dict(aliases),
        out_shape=outs,
        scratch_shapes=scratch,
        name=name,
    )(*operands)


def shards(
    prompt_layer_input,
    next_token_input,
    value_projection,
    output_gate_matrix,
    key_projection,
    query_projection,
    step_projection,
    value_filter_taps,
    key_filter_taps,
    query_filter_taps,
    step_size_bias,
    head_decay_logarithm,
    direct_path_weight,
    gated_norm_gain,
    position_decay_offset,
):
    prompts, length, width = prompt_layer_input.shape
    dests = lax.axis_size("sp")
    keep = P_SIZE // dests
    padded = -(-prompts // 8) * 8
    bias = step_size_bias[None]
    decay_rate = head_decay_logarithm[None]
    skip = direct_path_weight[None]
    out = jax.ShapeDtypeStruct
    value_rows = value_projection.T
    gate_rows = output_gate_matrix.T
    step_rows = step_projection.T
    offset_rows = jnp.swapaxes(position_decay_offset, 1, 2)

    per = 2
    local_outs = [
        out((prompts, P_SIZE, STATE), F32),
        out((CONV - 1, padded, 2 * LANES), F32),
        out((padded, length), F32),
        out((padded, LANES), F32),
    ]
    local_operands = (
        prompt_layer_input,
        key_projection,
        value_rows,
        step_rows,
        offset_rows,
    )
    away = [pl.BlockSpec(memory_space=pl.ANY)]
    local_scratch = [
        pltpu.VMEM((prompts, length, width), BF16),
        pltpu.VMEM((width, 2 * LANES), BF16),
        pltpu.VMEM(value_rows.shape, BF16),
        pltpu.VMEM(step_rows.shape, BF16),
        pltpu.VMEM(offset_rows.shape, F32),
        pltpu.VMEM((prompts, P_SIZE, length), F32),
        pltpu.VMEM((prompts, length, STATE), BF16),
        pltpu.VMEM((2, padded, length), F32),
        *[pltpu.VMEM(result.shape, result.dtype) for result in local_outs],
        pltpu.SemaphoreType.DMA((4,)),
        pltpu.SemaphoreType.DMA((prompts // per,)),
    ]
    *early, taps = call(
        lambda *refs: early_body(*refs, per=per),
        [*local_outs, out((8, 2 * LANES), F32)],
        *local_operands,
        value_filter_taps,
        key_filter_taps,
        bias,
        decay_rate,
        specs=away * 5 + whole(4),
        out_specs=away * 4 + whole(1),
        scratch=local_scratch,
        name="early",
    )
    block = 16
    trail, newest, new_decay, new_gate = call(
        token_body,
        [
            out((CONV - 1, padded, 2 * LANES), BF16),
            out((dests, 2 * padded, LANES), BF16),
            out((padded, LANES), F32),
            out((padded, P_SIZE), F32),
        ],
        prompt_layer_input,
        value_rows,
        gate_rows,
        step_rows,
        key_projection,
        query_projection,
        next_token_input,
        taps,
        query_filter_taps,
        bias,
        decay_rate,
        skip,
        specs=away * 6 + whole(6),
        scratch=[
            pltpu.VMEM((prompts, block, width), BF16),
            pltpu.VMEM((2 * P_SIZE + step_rows.shape[0], width), BF16),
            pltpu.VMEM((width, 2 * STATE), BF16),
            pltpu.VMEM((padded, width), F32),
            pltpu.VMEM((CONV - 1, padded, 3 * LANES), F32),
            pltpu.SemaphoreType.DMA((6,)),
        ],
        name="token",
    )
    newest = lax.all_to_all(newest, "sp", 0, 0, tiled=True)
    halo = lax.ppermute(trail, "sp", [(i, i + 1) for i in range(dests - 1)])
    state, lead, weight, logs = call(
        lambda *refs: late_body(*refs, per=per),
        local_outs,
        *local_operands,
        taps,
        bias,
        decay_rate,
        new_decay,
        *early,
        specs=away * 5 + whole(3) + away * 5,
        out_specs=away * 4,
        scratch=local_scratch,
        aliases=((9 + i, i) for i in range(4)),
        name="late",
    )
    (payload,) = call(
        pack_body,
        [out((dests, prompts * keep + padded, STATE), BF16)],
        halo,
        lead,
        weight,
        logs,
        taps,
        state,
        newest,
        name="pack",
    )
    received = lax.all_to_all(payload, "sp", 0, 0, tiled=True)
    tp_size = lax.axis_size(TP)
    cache, gated, squares = call(
        lambda *refs: read_body(*refs, prompts=prompts),
        [
            out((prompts * keep, STATE), BF16),
            out((8, LANES), F32),
            out((tp_size, 1, LANES), F32),
        ],
        received,
        newest,
        new_decay,
        new_gate,
        name="read",
    )
    squares = lax.all_to_all(squares, TP, 0, 0, tiled=True)
    (first_read,) = call(
        final_body, [out((1, keep, prompts), BF16)], squares, gated, gated_norm_gain, name="final"
    )
    return cache.reshape(prompts, 1, keep, STATE), jnp.transpose(first_read, (2, 0, 1))


def solution(mesh):
    split = Mesh(
        mesh.devices.reshape(mesh.shape["grp"], mesh.shape["sp"], mesh.shape["tp"] // 2, 2),
        ("grp", "sp", "tp_0", "tp_1"),
    )
    return jax.shard_map(
        shards,
        mesh=split,
        in_specs=(
            P("grp", "sp", None),
            P("grp", None),
            P(None, TP),
            P(None, TP),
            P(),
            P(),
            P(),
            P(),
            P(),
            P(),
            P(),
            P(),
            P(),
            P(),
            P("grp", "sp", None),
        ),
        out_specs=(P("grp", TP, "sp", None), P("grp", TP, "sp")),
        check_vma=False,
    )
```

```python
import jax
import jax.numpy as jnp
from jax import lax
from jax.experimental import pallas as pl
from jax.experimental.pallas import tpu as pltpu
from jax.sharding import Mesh
from jax.sharding import PartitionSpec as P

HEADS = 32
P_SIZE = 64
GROUPS = 2
STATE = 128
CONV = 4
LANES = 128
TP = ("tp_0", "tp_1")
EPSILON = 1e-06

F32 = jnp.float32
BF16 = jnp.bfloat16


def rounded(value):
    return value.astype(BF16).astype(F32)


def silu(value):
    return value / (1.0 + jnp.exp(-value))


def softplus(value):
    return jnp.maximum(value, 0.0) + jnp.log1p(jnp.exp(-jnp.abs(value)))


def dot(a, b, dims=((1,), (0,))):
    return lax.dot_general(a, b, (dims, ((), ())), preferred_element_type=F32)


def pieces(value):
    first = value.astype(BF16)
    rest = value - first.astype(F32)
    second = rest.astype(BF16)
    third = (rest - second.astype(F32)).astype(BF16)
    return first, second, third


def dot01(matrix, value):
    a, b, c = pieces(value)
    return dot(jnp.concatenate([matrix] * 3, axis=1), jnp.concatenate([a, b, c], axis=0))


def iota(shape, dim):
    return lax.broadcasted_iota(jnp.int32, shape, dim)


def own_half(row, head):
    return jnp.where(head % 2 == 0, row, pltpu.roll(row, 64, axis=1))


def pick(row, lane):
    return jnp.sum(jnp.where(iota(row.shape, 1) == lane, row, 0.0), axis=1, keepdims=True)


def pick_row(matrix, row):
    matrix = matrix.astype(F32)
    return jnp.sum(jnp.where(iota(matrix.shape, 0) == row, matrix, 0.0), axis=0, keepdims=True)


def local_body(
    x_hbm, key_hbm, value_hbm, step_hbm, off_hbm, vt_hbm, kt_hbm, bias_hbm, decay_hbm,
    state_hbm, lead_hbm, weight_hbm, logs_hbm,
    x_ref, w_ref, value_ref, step_ref, off_ref, vt_ref, kt_ref, bias_ref, decay_ref,
    wide_ref, map_ref, rows_ref, state_ref, lead_ref, weight_ref, logs_ref, small_sems, sems,
    *, per,
):
    prompts, length, width = x_hbm.shape
    head = lax.axis_index(TP)
    group = head // (HEADS // GROUPS)
    at = pl.multiple_of(group * STATE, STATE)
    small = (
        (value_hbm, value_ref),
        (step_hbm, step_ref),
        (key_hbm.at[:, pl.ds(at, STATE)], w_ref.at[:, pl.ds(LANES, STATE)]),
        (off_hbm, off_ref),
        (vt_hbm, vt_ref),
        (kt_hbm, kt_ref),
        (bias_hbm, bias_ref),
        (decay_hbm, decay_ref),
    )
    small = [pltpu.make_async_copy(*pair, small_sems.at[i]) for i, pair in enumerate(small)]
    for copy in small:
        copy.start()
    copies = []
    for i in range(prompts // per):
        part = pl.ds(i * per, per)
        copies.append(pltpu.make_async_copy(x_hbm.at[part], x_ref.at[part], sems.at[i]))
    for copy in copies:
        copy.start()
    small[0].wait()
    small[1].wait()
    step_row = jnp.broadcast_to(pick_row(step_ref[...], head), (P_SIZE, width)).astype(BF16)
    w_ref[:, :LANES] = jnp.transpose(jnp.concatenate([value_ref[...], step_row], axis=0))
    for copy in small[3:]:
        copy.wait()
    taps = taps_of(vt_ref, kt_ref)
    rows_ref[...] = jnp.zeros_like(rows_ref)
    offset = off_ref[...]
    offset = jnp.where(iota(offset.shape, 1) == head, offset, 0.0)
    rows_ref[1, :prompts] = jnp.sum(offset, axis=1)
    feature = iota((length, LANES), 1) < P_SIZE
    small[2].wait()
    for i in range(prompts // per):
        copies[i].wait()
        rows = x_ref[i * per : (i + 1) * per].reshape(per * length, width)
        raw_all = rounded(dot(rows, w_ref[...]))
        for j in range(per):
            b = i * per + j
            raw = raw_all[j * length : (j + 1) * length]
            for k in range(CONV - 1):
                lead_ref[k, b : b + 1, :] = raw[k : k + 1]
            total = raw * taps[CONV - 1 : CONV]
            for k in range(CONV - 1):
                total = total + pltpu.roll(raw, CONV - 1 - k, axis=0) * taps[k : k + 1]
            mixed = silu(total)
            map_ref[b] = mixed[:, LANES:].astype(BF16)
            turned = jnp.where(feature, rounded(mixed[:, :LANES]), raw[:, :LANES])
            turned = jnp.transpose(turned)
            wide_ref[b] = turned[:P_SIZE]
            rows_ref[0, b : b + 1, :] = turned[P_SIZE : P_SIZE + 1]
    step = softplus(rows_ref[0] + pick(bias_ref[...], head))
    log = rows_ref[1] - jnp.exp(pick(decay_ref[...], head)) * step
    later = (iota((length, length), 0) > iota((length, length), 1)).astype(BF16)
    after = dot(jnp.concatenate(pieces(log), axis=1), jnp.concatenate([later] * 3, axis=0))
    weight = jnp.exp(after) * step
    weight_ref[...] = weight
    logs_ref[...] = jnp.broadcast_to(jnp.sum(log, axis=1, keepdims=True), logs_ref.shape)
    weight = jnp.where(iota(weight.shape, 1) >= CONV - 1, weight, 0.0)
    for b in range(prompts):
        weighted = (wide_ref[b] * weight[b : b + 1]).astype(BF16)
        state_ref[b] = dot(weighted, map_ref[b])
    results = (
        (state_ref, state_hbm),
        (lead_ref, lead_hbm),
        (weight_ref, weight_hbm),
        (logs_ref, logs_hbm),
    )
    results = [pltpu.make_async_copy(*pair, small_sems.at[i]) for i, pair in enumerate(results)]
    for copy in results:
        copy.start()
    for copy in results:
        copy.wait()


def taps_of(vt_ref, kt_ref):
    head = lax.axis_index(TP)
    at = pl.multiple_of((head // (HEADS // GROUPS)) * STATE, STATE)
    pair = pl.multiple_of((head // 2) * LANES, LANES)
    value_taps = own_half(vt_ref[:, pl.ds(pair, LANES)].astype(F32), head)
    return jnp.concatenate([value_taps, kt_ref[:, pl.ds(at, STATE)].astype(F32)], axis=1)


def is_late():
    return lax.axis_index("sp") >= lax.axis_size("sp") - 2


def early_body(*refs, per):
    @pl.when(jnp.logical_not(is_late()))
    def _():
        local_body(*refs, per=per)


def late_body(*refs, operands, per):
    passed = operands + 5

    @pl.when(is_late())
    def _():
        local_body(*refs[:operands], *refs[passed:], per=per)


def token_body(
    x_hbm, value_hbm, gate_hbm, step_hbm, key_hbm, query_hbm, next_hbm, vt_hbm, kt_hbm, qt_hbm,
    bias_hbm, decay_hbm, skip_hbm, after_hbm,
    trail_ref, newest_ref, direct_ref, decay_out_ref, gate_out_ref,
    x_ref, rows_ref, maps_ref, next_ref, vt_ref, kt_ref, qt_ref, bias_ref, decay_ref, skip_ref,
    pad_ref, last_ref, sems,
):
    prompts, block, width = x_ref.shape
    head = lax.axis_index(TP)
    padded = pad_ref.shape[0]
    heads = step_hbm.shape[0]
    at = pl.multiple_of((head // (HEADS // GROUPS)) * STATE, STATE)
    tail = x_hbm.shape[1] - block
    copies = (
        (key_hbm.at[:, pl.ds(at, STATE)], maps_ref.at[:, pl.ds(0, STATE)]),
        (query_hbm.at[:, pl.ds(at, STATE)], maps_ref.at[:, pl.ds(STATE, STATE)]),
        (value_hbm, rows_ref.at[pl.ds(0, P_SIZE)]),
        (gate_hbm, rows_ref.at[pl.ds(P_SIZE, P_SIZE)]),
        (step_hbm, rows_ref.at[pl.ds(2 * P_SIZE, heads)]),
        (x_hbm.at[:, pl.ds(tail, block)], x_ref),
        (next_hbm, next_ref),
        (vt_hbm, vt_ref),
        (kt_hbm, kt_ref),
        (qt_hbm, qt_ref),
        (bias_hbm, bias_ref),
        (decay_hbm, decay_ref),
        (skip_hbm, skip_ref),
    )
    copies = [pltpu.make_async_copy(*pair, sems.at[i]) for i, pair in enumerate(copies)]
    for copy in copies:
        copy.start()
    for copy in copies:
        copy.wait()
    taps = taps_of(vt_ref, kt_ref)
    value_taps, key_taps = taps[:, :P_SIZE], taps[:, LANES:]
    query_taps = qt_ref[:, pl.ds(at, STATE)].astype(F32)
    pad_ref[...] = jnp.zeros_like(pad_ref)
    pad_ref[:prompts] = next_ref[...].astype(F32)
    token = pad_ref[...].astype(BF16)
    rows = jnp.concatenate([x_ref[...].reshape(prompts * block, width), token], axis=0)
    count = prompts * block
    maps = rounded(dot(rows, maps_ref[...]))
    keys, queries = maps[:, :STATE], maps[:, STATE:]
    others = rounded(dot(rows, rows_ref[...], ((1,), (1,))))
    values = others[:, :P_SIZE]
    new_gate = others[count:, P_SIZE : 2 * P_SIZE]
    new_step = pick(others[count:, 2 * P_SIZE :], head)
    last_ref[...] = jnp.zeros_like(last_ref)
    for b in range(prompts):
        at_row = (b + 1) * block - (CONV - 1)
        for k in range(CONV - 1):
            row = slice(at_row + k, at_row + k + 1)
            last_ref[k, b : b + 1, :P_SIZE] = values[row]
            last_ref[k, b : b + 1, LANES : 2 * LANES] = keys[row]
            last_ref[k, b : b + 1, 2 * LANES :] = queries[row]
    last = last_ref[...]
    trail_ref[...] = last[:, :, : 2 * LANES].astype(BF16)
    value_sum = last[0, :, :P_SIZE] * value_taps[:1]
    key_sum = last[0, :, LANES : 2 * LANES] * key_taps[:1]
    query_sum = last[0, :, 2 * LANES :] * query_taps[:1]
    for k in range(1, CONV - 1):
        value_sum = value_sum + last[k, :, :P_SIZE] * value_taps[k : k + 1]
        key_sum = key_sum + last[k, :, LANES : 2 * LANES] * key_taps[k : k + 1]
        query_sum = query_sum + last[k, :, 2 * LANES :] * query_taps[k : k + 1]
    new_input = rounded(silu(value_sum + values[count:] * value_taps[CONV - 1 : CONV]))
    new_in = rounded(silu(key_sum + keys[count:] * key_taps[CONV - 1 : CONV]))
    new_out = rounded(silu(query_sum + queries[count:] * query_taps[CONV - 1 : CONV]))
    step = softplus(new_step + pick(bias_ref[...], head))
    speed = jnp.exp(pick(decay_ref[...], head))
    decay_out_ref[...] = jnp.broadcast_to(jnp.exp(-speed * step), decay_out_ref.shape)
    agreement = jnp.sum(new_in * new_out, axis=1, keepdims=True)
    direct_ref[...] = new_input * (step * agreement + pick(skip_ref[...], head))
    newest = new_out.astype(BF16)
    for d in range(newest_ref.shape[0]):
        newest_ref[d] = newest
    gate_out_ref[...] = silu(new_gate)


def pack_body(
    halo_ref, lead_ref, weight_ref, logs_ref, vt_ref, kt_ref, state_ref, newest_ref, direct_ref,
    decay_ref, out_ref,
):
    prompts, rows, _ = state_ref.shape
    dests = out_ref.shape[0]
    keep = rows // dests
    padded = logs_ref.shape[0]
    taps = taps_of(vt_ref, kt_ref)
    new_out = newest_ref[dests - 1].astype(F32)
    window = [halo_ref[k].astype(F32) for k in range(CONV - 1)]
    window = window + [lead_ref[k] for k in range(CONV - 1)]
    weighted, maps = [], []
    for t in range(CONV - 1):
        total = window[t] * taps[:1]
        for k in range(1, CONV):
            total = total + window[t + k] * taps[k : k + 1]
        mixed = rounded(silu(total))
        weight = pick(weight_ref[...], t)
        weighted.append(jnp.transpose(rounded(mixed[:, :LANES] * weight)))
        maps.append(mixed[:, LANES:])
    states = []
    reads = jnp.zeros((rows, LANES), F32)
    lane = iota((rows, LANES), 1)
    for b in range(prompts):
        state = state_ref[b]
        for t in range(CONV - 1):
            state = state + weighted[t][:rows, b : b + 1] * maps[t][b : b + 1]
        states.append(state)
        read = jnp.sum(state * new_out[b : b + 1], axis=1, keepdims=True)
        reads = jnp.where(lane == b, read, reads)
    pair_rows = 2 * keep
    blocks = rows // pair_rows
    low = iota((blocks, pair_rows, STATE), 1) < keep
    for b in range(0, prompts, 2):
        one = states[b].reshape(blocks, pair_rows, STATE)
        two = states[b + 1].reshape(blocks, pair_rows, STATE)
        even = jnp.where(low, one, pltpu.roll(two, keep, axis=1))
        odd = jnp.where(low, pltpu.roll(one, keep, axis=1), two)
        at = b * keep
        for k in range(blocks):
            out_ref[2 * k, at : at + pair_rows, :] = even[k].astype(BF16)
            out_ref[2 * k + 1, at : at + pair_rows, :] = odd[k].astype(BF16)
    reads = jnp.transpose(reads)[:padded]
    on_last = lax.axis_index("sp") == dests - 1
    final = decay_ref[...] * reads[:, :P_SIZE] + direct_ref[...]
    reads = jnp.where(on_last, final, reads[:, :P_SIZE])
    high = rounded(reads)
    extra = jnp.concatenate([high, reads - high], axis=1)
    corner = (padded, LANES)
    logs = jnp.where(iota(corner, 0) == iota(corner, 1), logs_ref[...], 0.0)
    logs = jnp.sum(logs, axis=0, keepdims=True)
    for k, part in enumerate(pieces(logs)):
        extra = jnp.where(iota(corner, 0) == prompts + k, part.astype(F32), extra)
    extra = extra.astype(BF16)
    for d in range(dests):
        out_ref[d, prompts * keep :, :] = extra


def read_body(
    parts_ref, decay_ref, gate_ref, cache_ref, gated_ref, squares_ref, *, prompts,
):
    sources, _, _ = parts_ref.shape
    padded = decay_ref.shape[0]
    rows = parts_ref.shape[1] - padded
    keep = rows // prompts
    shard = lax.axis_index("sp")
    state_own = iota((rows, LANES), 1) == iota((rows, LANES), 0) // keep
    read_own = iota((padded, LANES), 1) == iota((padded, LANES), 0)
    total = jnp.zeros((rows, STATE), F32)
    reads = jnp.zeros((padded, P_SIZE), F32)
    for s in range(sources):
        extra = parts_ref[s, rows:, :].astype(F32)
        decay = jnp.sum(extra[prompts : prompts + 3], axis=0, keepdims=True)
        decay = jnp.exp(decay)
        per_row = jnp.sum(jnp.where(state_own, decay, 0.0), axis=1, keepdims=True)
        per_prompt = jnp.sum(jnp.where(read_own, decay, 0.0), axis=1, keepdims=True)
        total = total * per_row + parts_ref[s, :rows, :].astype(F32)
        reads = reads * per_prompt
        if s == sources - 1:
            reads = decay_ref[...] * reads
        reads = reads + (extra[:, :P_SIZE] + extra[:, P_SIZE:])
    cache_ref[...] = total.astype(BF16)
    gated = reads * gate_ref[...]
    gated = jnp.where(iota(gated.shape, 0) < prompts, gated, 0.0)
    squares = jnp.sum(gated * gated, axis=1, keepdims=True)
    squares = jnp.sum(jnp.where(read_own, squares, 0.0), axis=0, keepdims=True)
    squares_ref[...] = jnp.broadcast_to(squares[None], squares_ref.shape)
    square = jnp.concatenate([gated, jnp.zeros((P_SIZE - padded, P_SIZE), F32)], axis=0)
    square = jnp.concatenate([square, jnp.zeros((P_SIZE, P_SIZE), F32)], axis=0)
    square = jnp.concatenate([square, jnp.zeros((LANES, P_SIZE), F32)], axis=1)
    own = (iota((8, LANES), 1) == shard * keep + iota((8, LANES), 0)).astype(BF16)
    gated_ref[...] = dot01(own, jnp.transpose(square))


def final_body(parts_ref, gated_ref, gain_ref, out_ref):
    _, keep, prompts = out_ref.shape
    heads, rows = gain_ref.shape
    head = lax.axis_index(TP)
    shard = lax.axis_index("sp")
    total = jnp.sum(parts_ref[...], axis=0)
    scale = lax.rsqrt(total / (heads * rows) + EPSILON)
    gain = jnp.broadcast_to(pick_row(gain_ref[...], head), (8, rows))
    own = iota((8, rows), 1) == shard * keep + iota((8, rows), 0)
    gain = jnp.sum(jnp.where(own, gain, 0.0), axis=1, keepdims=True)
    out = gated_ref[...] * scale * gain
    out_ref[0] = out[:keep, :prompts].astype(BF16)


def whole(count):
    return [pl.BlockSpec(memory_space=pltpu.VMEM) for _ in range(count)]


def call(body, outs, *operands, specs=None, out_specs=None, scratch=(), aliases=(), name=None):
    return pl.pallas_call(
        body,
        in_specs=specs or whole(len(operands)),
        out_specs=out_specs or whole(len(outs)),
        input_output_aliases=dict(aliases),
        out_shape=outs,
        scratch_shapes=scratch,
        name=name,
    )(*operands)


def shards(
    prompt_layer_input,
    next_token_input,
    value_projection,
    output_gate_matrix,
    key_projection,
    query_projection,
    step_projection,
    value_filter_taps,
    key_filter_taps,
    query_filter_taps,
    step_size_bias,
    head_decay_logarithm,
    direct_path_weight,
    gated_norm_gain,
    position_decay_offset,
):
    prompts, length, width = prompt_layer_input.shape
    dests = lax.axis_size("sp")
    keep = P_SIZE // dests
    padded = -(-prompts // 8) * 8
    bias = step_size_bias[None]
    decay_rate = head_decay_logarithm[None]
    skip = direct_path_weight[None]
    out = jax.ShapeDtypeStruct
    value_rows = value_projection.T
    gate_rows = output_gate_matrix.T
    step_rows = step_projection.T
    offset_rows = jnp.swapaxes(position_decay_offset, 1, 2)

    per = 2
    local_outs = [
        out((prompts, P_SIZE, STATE), F32),
        out((CONV - 1, padded, 2 * LANES), F32),
        out((padded, length), F32),
        out((padded, LANES), F32),
    ]
    local_operands = (
        prompt_layer_input,
        key_projection,
        value_rows,
        step_rows,
        offset_rows,
        value_filter_taps,
        key_filter_taps,
        bias,
        decay_rate,
    )
    away = [pl.BlockSpec(memory_space=pl.ANY)]
    local_scratch = [
        pltpu.VMEM((prompts, length, width), BF16),
        pltpu.VMEM((width, 2 * LANES), BF16),
        pltpu.VMEM(value_rows.shape, BF16),
        pltpu.VMEM(step_rows.shape, BF16),
        pltpu.VMEM(offset_rows.shape, F32),
        pltpu.VMEM(value_filter_taps.shape, BF16),
        pltpu.VMEM(key_filter_taps.shape, BF16),
        pltpu.VMEM(bias.shape, F32),
        pltpu.VMEM(decay_rate.shape, F32),
        pltpu.VMEM((prompts, P_SIZE, length), F32),
        pltpu.VMEM((prompts, length, STATE), BF16),
        pltpu.VMEM((2, padded, length), F32),
        *[pltpu.VMEM(result.shape, result.dtype) for result in local_outs],
        pltpu.SemaphoreType.DMA((8,)),
        pltpu.SemaphoreType.DMA((prompts // per,)),
    ]
    early = call(
        lambda *refs: early_body(*refs, per=per),
        local_outs,
        *local_operands,
        specs=away * len(local_operands),
        out_specs=away * 4,
        scratch=local_scratch,
        name="early",
    )
    block = 16
    trail, newest, direct, new_decay, new_gate = call(
        token_body,
        [
            out((CONV - 1, padded, 2 * LANES), BF16),
            out((dests, padded, LANES), BF16),
            out((padded, P_SIZE), F32),
            out((padded, P_SIZE), F32),
            out((padded, P_SIZE), F32),
        ],
        prompt_layer_input,
        value_rows,
        gate_rows,
        step_rows,
        key_projection,
        query_projection,
        next_token_input,
        value_filter_taps,
        key_filter_taps,
        query_filter_taps,
        bias,
        decay_rate,
        skip,
        early[3],
        specs=away * 14,
        scratch=[
            pltpu.VMEM((prompts, block, width), BF16),
            pltpu.VMEM((2 * P_SIZE + step_rows.shape[0], width), BF16),
            pltpu.VMEM((width, 2 * STATE), BF16),
            pltpu.VMEM(next_token_input.shape, BF16),
            pltpu.VMEM(value_filter_taps.shape, BF16),
            pltpu.VMEM(key_filter_taps.shape, BF16),
            pltpu.VMEM(query_filter_taps.shape, BF16),
            pltpu.VMEM(bias.shape, F32),
            pltpu.VMEM(decay_rate.shape, F32),
            pltpu.VMEM(skip.shape, F32),
            pltpu.VMEM((padded, width), F32),
            pltpu.VMEM((CONV - 1, padded, 3 * LANES), F32),
            pltpu.SemaphoreType.DMA((13,)),
        ],
        name="token",
    )
    newest = lax.all_to_all(newest, "sp", 0, 0, tiled=True)
    halo = lax.ppermute(trail, "sp", [(i, i + 1) for i in range(dests - 1)])
    count = len(local_operands)
    state, lead, weight, logs = call(
        lambda *refs: late_body(*refs, operands=count, per=per),
        local_outs,
        *local_operands,
        new_decay,
        *early,
        specs=away * (count + 5),
        out_specs=away * 4,
        scratch=local_scratch,
        aliases=((count + 1 + i, i) for i in range(4)),
        name="late",
    )
    (payload,) = call(
        pack_body,
        [out((dests, prompts * keep + padded, STATE), BF16)],
        halo,
        lead,
        weight,
        logs,
        value_filter_taps,
        key_filter_taps,
        state,
        newest,
        direct,
        new_decay,
        name="pack",
    )
    received = lax.all_to_all(payload, "sp", 0, 0, tiled=True)
    tp_size = lax.axis_size(TP)
    cache, gated, squares = call(
        lambda *refs: read_body(*refs, prompts=prompts),
        [
            out((prompts * keep, STATE), BF16),
            out((8, LANES), F32),
            out((tp_size, 1, LANES), F32),
        ],
        received,
        new_decay,
        new_gate,
        name="read",
    )
    squares = lax.all_to_all(squares, TP, 0, 0, tiled=True)
    (first_read,) = call(
        final_body, [out((1, keep, prompts), BF16)], squares, gated, gated_norm_gain, name="final"
    )
    return cache.reshape(prompts, 1, keep, STATE), jnp.transpose(first_read, (2, 0, 1))


def solution(mesh):
    split = Mesh(
        mesh.devices.reshape(mesh.shape["grp"], mesh.shape["sp"], mesh.shape["tp"] // 2, 2),
        ("grp", "sp", "tp_0", "tp_1"),
    )
    return jax.shard_map(
        shards,
        mesh=split,
        in_specs=(
            P("grp", "sp", None),
            P("grp", None),
            P(None, TP),
            P(None, TP),
            P(),
            P(),
            P(),
            P(),
            P(),
            P(),
            P(),
            P(),
            P(),
            P(),
            P("grp", "sp", None),
        ),
        out_specs=(P("grp", TP, "sp", None), P("grp", TP, "sp")),
        check_vma=False,
    )
```

```python
import jax
import jax.numpy as jnp
from jax import lax
from jax.experimental import pallas as pl
from jax.experimental.pallas import tpu as pltpu
from jax.sharding import Mesh
from jax.sharding import PartitionSpec as P

HEADS = 32
P_SIZE = 64
GROUPS = 2
STATE = 128
CONV = 4
LANES = 128
TP = ("tp_0", "tp_1")
EPSILON = 1e-06

F32 = jnp.float32
BF16 = jnp.bfloat16


def rounded(value):
    return value.astype(BF16).astype(F32)


def silu(value):
    return value / (1.0 + jnp.exp(-value))


def softplus(value):
    return jnp.maximum(value, 0.0) + jnp.log1p(jnp.exp(-jnp.abs(value)))


def dot(a, b, dims=((1,), (0,))):
    return lax.dot_general(a, b, (dims, ((), ())), preferred_element_type=F32)


def pieces(value):
    first = value.astype(BF16)
    rest = value - first.astype(F32)
    second = rest.astype(BF16)
    third = (rest - second.astype(F32)).astype(BF16)
    return first, second, third


def dot01(matrix, value):
    a, b, c = pieces(value)
    return dot(jnp.concatenate([matrix] * 3, axis=1), jnp.concatenate([a, b, c], axis=0))


def iota(shape, dim):
    return lax.broadcasted_iota(jnp.int32, shape, dim)


def own_half(row, head):
    return jnp.where(head % 2 == 0, row, pltpu.roll(row, 64, axis=1))


def pick(row, lane):
    return jnp.sum(jnp.where(iota(row.shape, 1) == lane, row, 0.0), axis=1, keepdims=True)


def pick_row(matrix, row):
    matrix = matrix.astype(F32)
    return jnp.sum(jnp.where(iota(matrix.shape, 0) == row, matrix, 0.0), axis=0, keepdims=True)


def local_body(
    x_hbm, key_hbm, value_hbm, step_hbm, off_hbm, vt_hbm, kt_hbm, bias_hbm, decay_hbm,
    state_hbm, lead_hbm, weight_hbm, logs_hbm,
    x_ref, w_ref, value_ref, step_ref, off_ref, vt_ref, kt_ref, bias_ref, decay_ref,
    wide_ref, map_ref, rows_ref, state_ref, lead_ref, weight_ref, logs_ref, small_sems, sems,
    *, per,
):
    prompts, length, width = x_hbm.shape
    head = lax.axis_index(TP)
    group = head // (HEADS // GROUPS)
    at = pl.multiple_of(group * STATE, STATE)
    small = (
        (value_hbm, value_ref),
        (step_hbm, step_ref),
        (key_hbm.at[:, pl.ds(at, STATE)], w_ref.at[:, pl.ds(LANES, STATE)]),
        (off_hbm, off_ref),
        (vt_hbm, vt_ref),
        (kt_hbm, kt_ref),
        (bias_hbm, bias_ref),
        (decay_hbm, decay_ref),
    )
    small = [pltpu.make_async_copy(*pair, small_sems.at[i]) for i, pair in enumerate(small)]
    for copy in small:
        copy.start()
    copies = []
    for i in range(prompts // per):
        part = pl.ds(i * per, per)
        copies.append(pltpu.make_async_copy(x_hbm.at[part], x_ref.at[part], sems.at[i]))
    for copy in copies:
        copy.start()
    small[0].wait()
    small[1].wait()
    step_row = jnp.broadcast_to(pick_row(step_ref[...], head), (P_SIZE, width)).astype(BF16)
    w_ref[:, :LANES] = jnp.transpose(jnp.concatenate([value_ref[...], step_row], axis=0))
    for copy in small[3:]:
        copy.wait()
    taps = taps_of(vt_ref, kt_ref)
    rows_ref[...] = jnp.zeros_like(rows_ref)
    offset = off_ref[...]
    offset = jnp.where(iota(offset.shape, 1) == head, offset, 0.0)
    rows_ref[1, :prompts] = jnp.sum(offset, axis=1)
    feature = iota((length, LANES), 1) < P_SIZE
    small[2].wait()
    for i in range(prompts // per):
        copies[i].wait()
        rows = x_ref[i * per : (i + 1) * per].reshape(per * length, width)
        raw_all = rounded(dot(rows, w_ref[...]))
        for j in range(per):
            b = i * per + j
            raw = raw_all[j * length : (j + 1) * length]
            for k in range(CONV - 1):
                lead_ref[k, b : b + 1, :] = raw[k : k + 1]
            total = raw * taps[CONV - 1 : CONV]
            for k in range(CONV - 1):
                total = total + pltpu.roll(raw, CONV - 1 - k, axis=0) * taps[k : k + 1]
            mixed = silu(total)
            map_ref[b] = mixed[:, LANES:].astype(BF16)
            turned = jnp.where(feature, rounded(mixed[:, :LANES]), raw[:, :LANES])
            turned = jnp.transpose(turned)
            wide_ref[b] = turned[:P_SIZE]
            rows_ref[0, b : b + 1, :] = turned[P_SIZE : P_SIZE + 1]
    step = softplus(rows_ref[0] + pick(bias_ref[...], head))
    log = rows_ref[1] - jnp.exp(pick(decay_ref[...], head)) * step
    later = (iota((length, length), 0) > iota((length, length), 1)).astype(BF16)
    after = dot(jnp.concatenate(pieces(log), axis=1), jnp.concatenate([later] * 3, axis=0))
    weight = jnp.exp(after) * step
    weight_ref[...] = weight
    logs_ref[...] = jnp.broadcast_to(jnp.sum(log, axis=1, keepdims=True), logs_ref.shape)
    weight = jnp.where(iota(weight.shape, 1) >= CONV - 1, weight, 0.0)
    for b in range(prompts):
        weighted = (wide_ref[b] * weight[b : b + 1]).astype(BF16)
        state_ref[b] = dot(weighted, map_ref[b])
    results = (
        (state_ref, state_hbm),
        (lead_ref, lead_hbm),
        (weight_ref, weight_hbm),
        (logs_ref, logs_hbm),
    )
    results = [pltpu.make_async_copy(*pair, small_sems.at[i]) for i, pair in enumerate(results)]
    for copy in results:
        copy.start()
    for copy in results:
        copy.wait()


def taps_of(vt_ref, kt_ref):
    head = lax.axis_index(TP)
    at = pl.multiple_of((head // (HEADS // GROUPS)) * STATE, STATE)
    pair = pl.multiple_of((head // 2) * LANES, LANES)
    value_taps = own_half(vt_ref[:, pl.ds(pair, LANES)].astype(F32), head)
    return jnp.concatenate([value_taps, kt_ref[:, pl.ds(at, STATE)].astype(F32)], axis=1)


def is_late():
    return lax.axis_index("sp") >= lax.axis_size("sp") - 2


def early_body(*refs, per):
    @pl.when(jnp.logical_not(is_late()))
    def _():
        local_body(*refs, per=per)


def late_body(*refs, operands, per):
    passed = operands + 5

    @pl.when(is_late())
    def _():
        local_body(*refs[:operands], *refs[passed:], per=per)


def token_body(
    x_hbm, value_hbm, gate_hbm, step_hbm, key_hbm, query_hbm, next_hbm, vt_hbm, kt_hbm, qt_hbm,
    bias_hbm, decay_hbm, skip_hbm, after_hbm,
    trail_ref, newest_ref, direct_ref, decay_out_ref, gate_out_ref,
    x_ref, rows_ref, maps_ref, next_ref, vt_ref, kt_ref, qt_ref, bias_ref, decay_ref, skip_ref,
    pad_ref, last_ref, sems,
):
    prompts, block, width = x_ref.shape
    head = lax.axis_index(TP)
    padded = pad_ref.shape[0]
    heads = step_hbm.shape[0]
    at = pl.multiple_of((head // (HEADS // GROUPS)) * STATE, STATE)
    tail = x_hbm.shape[1] - block
    copies = (
        (key_hbm.at[:, pl.ds(at, STATE)], maps_ref.at[:, pl.ds(0, STATE)]),
        (query_hbm.at[:, pl.ds(at, STATE)], maps_ref.at[:, pl.ds(STATE, STATE)]),
        (value_hbm, rows_ref.at[pl.ds(0, P_SIZE)]),
        (gate_hbm, rows_ref.at[pl.ds(P_SIZE, P_SIZE)]),
        (step_hbm, rows_ref.at[pl.ds(2 * P_SIZE, heads)]),
        (x_hbm.at[:, pl.ds(tail, block)], x_ref),
        (next_hbm, next_ref),
        (vt_hbm, vt_ref),
        (kt_hbm, kt_ref),
        (qt_hbm, qt_ref),
        (bias_hbm, bias_ref),
        (decay_hbm, decay_ref),
        (skip_hbm, skip_ref),
    )
    copies = [pltpu.make_async_copy(*pair, sems.at[i]) for i, pair in enumerate(copies)]
    for copy in copies:
        copy.start()
    for copy in copies:
        copy.wait()
    taps = taps_of(vt_ref, kt_ref)
    value_taps, key_taps = taps[:, :P_SIZE], taps[:, LANES:]
    query_taps = qt_ref[:, pl.ds(at, STATE)].astype(F32)
    pad_ref[...] = jnp.zeros_like(pad_ref)
    pad_ref[:prompts] = next_ref[...].astype(F32)
    token = pad_ref[...].astype(BF16)
    rows = jnp.concatenate([x_ref[...].reshape(prompts * block, width), token], axis=0)
    count = prompts * block
    maps = rounded(dot(rows, maps_ref[...]))
    keys, queries = maps[:, :STATE], maps[:, STATE:]
    others = rounded(dot(rows, rows_ref[...], ((1,), (1,))))
    values = others[:, :P_SIZE]
    new_gate = others[count:, P_SIZE : 2 * P_SIZE]
    new_step = pick(others[count:, 2 * P_SIZE :], head)
    last_ref[...] = jnp.zeros_like(last_ref)
    for b in range(prompts):
        at_row = (b + 1) * block - (CONV - 1)
        for k in range(CONV - 1):
            row = slice(at_row + k, at_row + k + 1)
            last_ref[k, b : b + 1, :P_SIZE] = values[row]
            last_ref[k, b : b + 1, LANES : 2 * LANES] = keys[row]
            last_ref[k, b : b + 1, 2 * LANES :] = queries[row]
    last = last_ref[...]
    trail_ref[...] = last[:, :, : 2 * LANES].astype(BF16)
    value_sum = last[0, :, :P_SIZE] * value_taps[:1]
    key_sum = last[0, :, LANES : 2 * LANES] * key_taps[:1]
    query_sum = last[0, :, 2 * LANES :] * query_taps[:1]
    for k in range(1, CONV - 1):
        value_sum = value_sum + last[k, :, :P_SIZE] * value_taps[k : k + 1]
        key_sum = key_sum + last[k, :, LANES : 2 * LANES] * key_taps[k : k + 1]
        query_sum = query_sum + last[k, :, 2 * LANES :] * query_taps[k : k + 1]
    new_input = rounded(silu(value_sum + values[count:] * value_taps[CONV - 1 : CONV]))
    new_in = rounded(silu(key_sum + keys[count:] * key_taps[CONV - 1 : CONV]))
    new_out = rounded(silu(query_sum + queries[count:] * query_taps[CONV - 1 : CONV]))
    step = softplus(new_step + pick(bias_ref[...], head))
    speed = jnp.exp(pick(decay_ref[...], head))
    decay_out_ref[...] = jnp.broadcast_to(jnp.exp(-speed * step), decay_out_ref.shape)
    agreement = jnp.sum(new_in * new_out, axis=1, keepdims=True)
    direct_ref[...] = new_input * (step * agreement + pick(skip_ref[...], head))
    newest = new_out[:prompts].astype(BF16)
    for d in range(newest_ref.shape[0]):
        newest_ref[d] = newest
    gate_out_ref[...] = silu(new_gate)


def pack_body(
    halo_ref, lead_ref, weight_ref, logs_ref, vt_ref, kt_ref, state_ref, newest_ref, direct_ref,
    decay_ref, out_ref,
):
    prompts, rows, _ = state_ref.shape
    dests = out_ref.shape[0]
    keep = rows // dests
    padded = logs_ref.shape[0]
    taps = taps_of(vt_ref, kt_ref)
    new_out = newest_ref[dests - 1].astype(F32)
    window = [halo_ref[k].astype(F32) for k in range(CONV - 1)]
    window = window + [lead_ref[k] for k in range(CONV - 1)]
    weighted, maps = [], []
    for t in range(CONV - 1):
        total = window[t] * taps[:1]
        for k in range(1, CONV):
            total = total + window[t + k] * taps[k : k + 1]
        mixed = rounded(silu(total))
        weight = pick(weight_ref[...], t)
        weighted.append(jnp.transpose(rounded(mixed[:, :LANES] * weight)))
        maps.append(mixed[:, LANES:])
    states = []
    reads = jnp.zeros((rows, LANES), F32)
    lane = iota((rows, LANES), 1)
    for b in range(prompts):
        state = state_ref[b]
        for t in range(CONV - 1):
            state = state + weighted[t][:rows, b : b + 1] * maps[t][b : b + 1]
        states.append(state)
        read = jnp.sum(state * new_out[b : b + 1], axis=1, keepdims=True)
        reads = jnp.where(lane == b, read, reads)
    pair_rows = 2 * keep
    blocks = rows // pair_rows
    low = iota((blocks, pair_rows, STATE), 1) < keep
    for b in range(0, prompts, 2):
        one = states[b].reshape(blocks, pair_rows, STATE)
        two = states[b + 1].reshape(blocks, pair_rows, STATE)
        even = jnp.where(low, one, pltpu.roll(two, keep, axis=1))
        odd = jnp.where(low, pltpu.roll(one, keep, axis=1), two)
        at = b * keep
        for k in range(blocks):
            out_ref[2 * k, at : at + pair_rows, :] = even[k].astype(BF16)
            out_ref[2 * k + 1, at : at + pair_rows, :] = odd[k].astype(BF16)
    reads = jnp.transpose(reads)[:padded]
    on_last = lax.axis_index("sp") == dests - 1
    final = decay_ref[...] * reads[:, :P_SIZE] + direct_ref[...]
    reads = jnp.where(on_last, final, reads[:, :P_SIZE])
    high = rounded(reads)
    extra = jnp.concatenate([high, reads - high], axis=1)
    corner = (padded, LANES)
    logs = jnp.where(iota(corner, 0) == iota(corner, 1), logs_ref[...], 0.0)
    logs = jnp.sum(logs, axis=0, keepdims=True)
    for k, part in enumerate(pieces(logs)):
        extra = jnp.where(iota(corner, 0) == prompts + k, part.astype(F32), extra)
    extra = extra.astype(BF16)
    for d in range(dests):
        out_ref[d, prompts * keep :, :] = extra


def read_body(
    parts_ref, decay_ref, gate_ref, cache_ref, gated_ref, squares_ref, *, prompts,
):
    sources, _, _ = parts_ref.shape
    padded = decay_ref.shape[0]
    rows = parts_ref.shape[1] - padded
    keep = rows // prompts
    shard = lax.axis_index("sp")
    state_own = iota((rows, LANES), 1) == iota((rows, LANES), 0) // keep
    read_own = iota((padded, LANES), 1) == iota((padded, LANES), 0)
    total = jnp.zeros((rows, STATE), F32)
    reads = jnp.zeros((padded, P_SIZE), F32)
    for s in range(sources):
        extra = parts_ref[s, rows:, :].astype(F32)
        decay = jnp.sum(extra[prompts : prompts + 3], axis=0, keepdims=True)
        decay = jnp.exp(decay)
        per_row = jnp.sum(jnp.where(state_own, decay, 0.0), axis=1, keepdims=True)
        per_prompt = jnp.sum(jnp.where(read_own, decay, 0.0), axis=1, keepdims=True)
        total = total * per_row + parts_ref[s, :rows, :].astype(F32)
        reads = reads * per_prompt
        if s == sources - 1:
            reads = decay_ref[...] * reads
        reads = reads + (extra[:, :P_SIZE] + extra[:, P_SIZE:])
    cache_ref[...] = total.astype(BF16)
    gated = reads * gate_ref[...]
    gated = jnp.where(iota(gated.shape, 0) < prompts, gated, 0.0)
    squares = jnp.sum(gated * gated, axis=1, keepdims=True)
    squares = jnp.sum(jnp.where(read_own, squares, 0.0), axis=0, keepdims=True)
    squares_ref[...] = jnp.broadcast_to(squares[None], squares_ref.shape)
    square = jnp.concatenate([gated, jnp.zeros((P_SIZE - padded, P_SIZE), F32)], axis=0)
    square = jnp.concatenate([square, jnp.zeros((P_SIZE, P_SIZE), F32)], axis=0)
    square = jnp.concatenate([square, jnp.zeros((LANES, P_SIZE), F32)], axis=1)
    own = (iota((8, LANES), 1) == shard * keep + iota((8, LANES), 0)).astype(BF16)
    gated_ref[...] = dot01(own, jnp.transpose(square))


def final_body(parts_ref, gated_ref, gain_ref, out_ref):
    _, keep, prompts = out_ref.shape
    heads, rows = gain_ref.shape
    head = lax.axis_index(TP)
    shard = lax.axis_index("sp")
    total = jnp.sum(parts_ref[...], axis=0)
    scale = lax.rsqrt(total / (heads * rows) + EPSILON)
    gain = jnp.broadcast_to(pick_row(gain_ref[...], head), (8, rows))
    own = iota((8, rows), 1) == shard * keep + iota((8, rows), 0)
    gain = jnp.sum(jnp.where(own, gain, 0.0), axis=1, keepdims=True)
    out = gated_ref[...] * scale * gain
    out_ref[0] = out[:keep, :prompts].astype(BF16)


def whole(count):
    return [pl.BlockSpec(memory_space=pltpu.VMEM) for _ in range(count)]


def call(body, outs, *operands, specs=None, out_specs=None, scratch=(), aliases=(), name=None):
    return pl.pallas_call(
        body,
        in_specs=specs or whole(len(operands)),
        out_specs=out_specs or whole(len(outs)),
        input_output_aliases=dict(aliases),
        out_shape=outs,
        scratch_shapes=scratch,
        name=name,
    )(*operands)


def shards(
    prompt_layer_input,
    next_token_input,
    value_projection,
    output_gate_matrix,
    key_projection,
    query_projection,
    step_projection,
    value_filter_taps,
    key_filter_taps,
    query_filter_taps,
    step_size_bias,
    head_decay_logarithm,
    direct_path_weight,
    gated_norm_gain,
    position_decay_offset,
):
    prompts, length, width = prompt_layer_input.shape
    dests = lax.axis_size("sp")
    keep = P_SIZE // dests
    padded = -(-prompts // 8) * 8
    bias = step_size_bias[None]
    decay_rate = head_decay_logarithm[None]
    skip = direct_path_weight[None]
    out = jax.ShapeDtypeStruct
    value_rows = value_projection.T
    gate_rows = output_gate_matrix.T
    step_rows = step_projection.T
    offset_rows = jnp.swapaxes(position_decay_offset, 1, 2)

    per = 2
    local_outs = [
        out((prompts, P_SIZE, STATE), F32),
        out((CONV - 1, padded, 2 * LANES), F32),
        out((padded, length), F32),
        out((padded, LANES), F32),
    ]
    local_operands = (
        prompt_layer_input,
        key_projection,
        value_rows,
        step_rows,
        offset_rows,
        value_filter_taps,
        key_filter_taps,
        bias,
        decay_rate,
    )
    away = [pl.BlockSpec(memory_space=pl.ANY)]
    local_scratch = [
        pltpu.VMEM((prompts, length, width), BF16),
        pltpu.VMEM((width, 2 * LANES), BF16),
        pltpu.VMEM(value_rows.shape, BF16),
        pltpu.VMEM(step_rows.shape, BF16),
        pltpu.VMEM(offset_rows.shape, F32),
        pltpu.VMEM(value_filter_taps.shape, BF16),
        pltpu.VMEM(key_filter_taps.shape, BF16),
        pltpu.VMEM(bias.shape, F32),
        pltpu.VMEM(decay_rate.shape, F32),
        pltpu.VMEM((prompts, P_SIZE, length), F32),
        pltpu.VMEM((prompts, length, STATE), BF16),
        pltpu.VMEM((2, padded, length), F32),
        *[pltpu.VMEM(result.shape, result.dtype) for result in local_outs],
        pltpu.SemaphoreType.DMA((8,)),
        pltpu.SemaphoreType.DMA((prompts // per,)),
    ]
    early = call(
        lambda *refs: early_body(*refs, per=per),
        local_outs,
        *local_operands,
        specs=away * len(local_operands),
        out_specs=away * 4,
        scratch=local_scratch,
        name="early",
    )
    block = 16
    trail, newest, direct, new_decay, new_gate = call(
        token_body,
        [
            out((CONV - 1, padded, 2 * LANES), BF16),
            out((dests, prompts, LANES), BF16),
            out((padded, P_SIZE), F32),
            out((padded, P_SIZE), F32),
            out((padded, P_SIZE), F32),
        ],
        prompt_layer_input,
        value_rows,
        gate_rows,
        step_rows,
        key_projection,
        query_projection,
        next_token_input,
        value_filter_taps,
        key_filter_taps,
        query_filter_taps,
        bias,
        decay_rate,
        skip,
        early[3],
        specs=away * 14,
        scratch=[
            pltpu.VMEM((prompts, block, width), BF16),
            pltpu.VMEM((2 * P_SIZE + step_rows.shape[0], width), BF16),
            pltpu.VMEM((width, 2 * STATE), BF16),
            pltpu.VMEM(next_token_input.shape, BF16),
            pltpu.VMEM(value_filter_taps.shape, BF16),
            pltpu.VMEM(key_filter_taps.shape, BF16),
            pltpu.VMEM(query_filter_taps.shape, BF16),
            pltpu.VMEM(bias.shape, F32),
            pltpu.VMEM(decay_rate.shape, F32),
            pltpu.VMEM(skip.shape, F32),
            pltpu.VMEM((padded, width), F32),
            pltpu.VMEM((CONV - 1, padded, 3 * LANES), F32),
            pltpu.SemaphoreType.DMA((13,)),
        ],
        name="token",
    )
    newest = lax.all_to_all(newest, "sp", 0, 0, tiled=True)
    halo = lax.ppermute(trail, "sp", [(i, i + 1) for i in range(dests - 1)])
    count = len(local_operands)
    state, lead, weight, logs = call(
        lambda *refs: late_body(*refs, operands=count, per=per),
        local_outs,
        *local_operands,
        new_decay,
        *early,
        specs=away * (count + 5),
        out_specs=away * 4,
        scratch=local_scratch,
        aliases=((count + 1 + i, i) for i in range(4)),
        name="late",
    )
    (payload,) = call(
        pack_body,
        [out((dests, prompts * keep + padded, STATE), BF16)],
        halo,
        lead,
        weight,
        logs,
        value_filter_taps,
        key_filter_taps,
        state,
        newest,
        direct,
        new_decay,
        name="pack",
    )
    received = lax.all_to_all(payload, "sp", 0, 0, tiled=True)
    tp_size = lax.axis_size(TP)
    cache, gated, squares = call(
        lambda *refs: read_body(*refs, prompts=prompts),
        [
            out((prompts * keep, STATE), BF16),
            out((8, LANES), F32),
            out((tp_size, 1, LANES), F32),
        ],
        received,
        new_decay,
        new_gate,
        name="read",
    )
    squares = lax.all_to_all(squares, TP, 0, 0, tiled=True)
    (first_read,) = call(
        final_body, [out((1, keep, prompts), BF16)], squares, gated, gated_norm_gain, name="final"
    )
    return cache.reshape(prompts, 1, keep, STATE), jnp.transpose(first_read, (2, 0, 1))


def solution(mesh):
    split = Mesh(
        mesh.devices.reshape(mesh.shape["grp"], mesh.shape["sp"], mesh.shape["tp"] // 2, 2),
        ("grp", "sp", "tp_0", "tp_1"),
    )
    return jax.shard_map(
        shards,
        mesh=split,
        in_specs=(
            P("grp", "sp", None),
            P("grp", None),
            P(None, TP),
            P(None, TP),
            P(),
            P(),
            P(),
            P(),
            P(),
            P(),
            P(),
            P(),
            P(),
            P(),
            P("grp", "sp", None),
        ),
        out_specs=(P("grp", TP, "sp", None), P("grp", TP, "sp")),
        check_vma=False,
    )
```
